32 devices in a mesh: sp: 8 (over z, y), tp: 4 (over x, core).
Axes of the slice: x: 2, y: 2, z: 4, core: 2. Of those that a mesh axis runs over, the one named last changes fastest.
Arguments:
- block_input: bfloat16 [8192, 2048], P('sp'), may hold values from -6 to 6
- out_grad: bfloat16 [8192, 2048], P('sp'), may hold values from -6 to 6
- w_value: bfloat16 [2048, 1024], P(None, 'tp'), may hold values from -0.125 to 0.125
- w_gate: bfloat16 [2048, 1024], P(None, 'tp'), may hold values from -0.125 to 0.125
- conv_taps: float32 [31, 1024], P(None, 'tp'), may hold values from -4 to 4
- norm_gain: float32 [1024], P('tp'), may hold values from 0.1 to 1.9
- norm_shift: float32 [1024], P('tp'), may hold values from -3 to 3
- w_proj: bfloat16 [1024, 2048], P('tp'), may hold values from -0.1875 to 0.1875
Outputs:
- input_grad: bfloat16 [8192, 2048], P('sp', 'tp')
- value_wgrad: float32 [2048, 1024], P('sp', 'tp')
- gate_wgrad: float32 [2048, 1024], P('sp', 'tp')
- proj_wgrad: float32 [1024, 2048], P('tp', 'sp')
- taps_grad: float32 [31, 1024], P(None, 'tp')
- gain_grad: float32 [1024], P('tp')
- shift_grad: float32 [1024], P('tp')
The draws below stay inside these ranges and needn't reach their ends.
All inputs are finite; a program needn't handle non-finite values.
Results may differ from the reference program's by a relative error of at most 0.014.
Values may be sent and summed in bfloat16 or wider, within the bound.
No kernel may reach another device: no remote copies, remote signals or barrier semaphores. Data moves between devices by JAX's collectives and lax.ppermute only.
A program may use at most 128 MiB of HBM per device.

```python
import math
import jax
import jax.numpy as jnp
from jax import lax

D = 2048
CH = 1024
KERNEL = 31
TOKENS = 8192
N_TP = 4


def draw_conv_taps(key, part):
    base = jax.random.fold_in(key, 11)
    first, second, third = jax.random.split(base, 3)
    channel = jnp.arange(CH, dtype=jnp.float32)
    phase = jax.random.uniform(first, (), jnp.float32, 0.0, 6.2831)
    level = jnp.exp(1.2 * jnp.sin(6.2831853 * channel / CH + phase))
    rough = jnp.exp(jax.random.uniform(second, (CH,), jnp.float32, -0.7, 0.7))
    taps = jax.random.truncated_normal(third, -3.0, 3.0, (KERNEL, CH), jnp.float32)
    return (taps * (level * rough)[None, :] / math.sqrt(KERNEL)).astype(jnp.float32)


def with_spikes(entries, rng, source, target, parts, factor):
    def block_of(dim):
        return (jnp.arange(entries.shape[dim]) // (entries.shape[dim] // parts)).reshape((-1,) + (1,) * (entries.ndim - 1 - dim))

    one_side = jax.random.permutation(rng, parts)[block_of(target)]
    other_side = (block_of(target) + parts // 2) % parts
    return jnp.where((block_of(source) == one_side) | (block_of(source) == other_side), factor * entries, entries)


def shard_levels(rng, dims, cuts, low, top_value):
    def one(dim, shards_of):
        steps = jax.random.uniform(jax.random.fold_in(jax.random.fold_in(rng, 6), dim), (shards_of,), jnp.float32, low / len(cuts), top_value / len(cuts))
        return jnp.repeat(jnp.exp(steps), dims[dim] // shards_of).reshape((-1,) + (1,) * (len(dims) - dim - 1))

    gain = one(*cuts[0])
    for cut in cuts[1:]:
        gain = gain * one(*cut)
    return gain


def scatter_about(stream_key, dims, spread, reach, pieces=(), kind=jnp.bfloat16):
    result = spread * jax.random.normal(stream_key, dims, jnp.float32)
    if pieces:
        result = result * shard_levels(stream_key, dims, pieces, -0.22, 0.18)
    return jnp.clip(result, -reach, reach).astype(kind)


def gaussian_with(own_key, dims, scale, limit, cuts, heavy, kind=jnp.bfloat16):
    entries = scale * jax.random.normal(own_key, dims, jnp.float32)
    if cuts:
        entries = entries * shard_levels(own_key, dims, cuts, -0.22, 0.18)
    return jnp.clip(with_spikes(entries, jax.random.fold_in(own_key, 3), *heavy), -limit, limit).astype(kind)


def setup_inputs(seed: int = 0) -> dict:
    streams_of = jax.random.split(jax.random.key(seed), 9)
    block_input = scatter_about(streams_of[0], (TOKENS, D), 1.0, 6.0, ((0, 8),))
    out_grad = gaussian_with(streams_of[1], (TOKENS, D), 1.0, 6.0, ((0, 8),), (0, 1, 8, 2.0))
    w_value = scatter_about(streams_of[2], (D, CH), D ** -0.5, 0.125, ((1, 4),))
    w_gate = scatter_about(streams_of[3], (D, CH), D ** -0.5, 0.125, ((1, 4),))
    conv_taps = draw_conv_taps(jax.random.fold_in(streams_of[8], 71), 0)
    norm_gain = jnp.clip(1.0 + 0.18 * jax.random.normal(streams_of[5], (CH,), jnp.float32), 0.1, 1.9)
    norm_shift = scatter_about(streams_of[6], (CH,), 0.5, 3.0, ((0, 4),), jnp.float32)
    w_proj = scatter_about(streams_of[7], (CH, D), CH ** -0.5, 0.1875, ((0, 4),))
    return {"block_input": block_input, "out_grad": out_grad, "w_value": w_value, "w_gate": w_gate, "conv_taps": conv_taps, "norm_gain": norm_gain, "norm_shift": norm_shift, "w_proj": w_proj}


EPS = 0.05

def reference(block_input, out_grad, w_value, w_gate, conv_taps, norm_gain, norm_shift, w_proj):
    value_proj = jnp.dot(block_input, w_value, preferred_element_type=jnp.float32).astype(jnp.bfloat16)
    gate_proj = jnp.dot(block_input, w_gate, preferred_element_type=jnp.float32).astype(jnp.bfloat16)
    gate_sigmoid = jax.nn.sigmoid(gate_proj.astype(jnp.float32))
    value_wide = value_proj.astype(jnp.float32)
    gated_input = (value_wide * gate_sigmoid).astype(jnp.bfloat16)
    padded_glu = jnp.pad(gated_input.astype(jnp.float32), ((KERNEL - 1, 0), (0, 0)))
    filtered = jnp.zeros((TOKENS, CH), jnp.float32)
    for tap_index in range(KERNEL):
        begin = KERNEL - 1 - tap_index
        filtered = filtered + conv_taps[tap_index] * padded_glu[begin:begin + TOKENS]
    row_mean = lax.optimization_barrier(jnp.sum(filtered, axis=1)) / CH
    row_var = lax.optimization_barrier(jnp.sum(filtered * filtered, axis=1)) / CH - row_mean * row_mean
    row_scale = lax.rsqrt(row_var + EPS)
    normed = (filtered - row_mean[:, None]) * row_scale[:, None]
    activated = normed * norm_gain + norm_shift
    act_sigmoid = jax.nn.sigmoid(activated)
    mixer_out = (activated * act_sigmoid).astype(jnp.bfloat16)
    grad_mixed = jnp.dot(out_grad, w_proj.T, preferred_element_type=jnp.float32)
    grad_act = grad_mixed * act_sigmoid * (1.0 + activated * (1.0 - act_sigmoid))
    grad_normed = grad_act * norm_gain
    first_mean = lax.optimization_barrier(jnp.sum(grad_normed, axis=1)) / CH
    second_mean = lax.optimization_barrier(jnp.sum(grad_normed * normed, axis=1)) / CH
    grad_filtered = row_scale[:, None] * (grad_normed - first_mean[:, None] - normed * second_mean[:, None])
    padded_grad = jnp.pad(grad_filtered, ((0, KERNEL - 1), (0, 0)))
    grad_glu = jnp.zeros((TOKENS, CH), jnp.float32)
    taps_rows = []
    for tap_index in range(KERNEL):
        begin = KERNEL - 1 - tap_index
        grad_glu = grad_glu + conv_taps[tap_index] * padded_grad[tap_index:tap_index + TOKENS]
        taps_rows.append(lax.optimization_barrier(jnp.sum(grad_filtered * padded_glu[begin:begin + TOKENS], axis=0)))
    grad_value = (grad_glu * gate_sigmoid).astype(jnp.bfloat16)
    grad_gate = (grad_glu * value_wide * gate_sigmoid * (1.0 - gate_sigmoid)).astype(jnp.bfloat16)
    block_cols = CH // N_TP
    summed = jnp.zeros((TOKENS, D), jnp.float32)
    for block_index in range(N_TP):
        low = block_index * block_cols
        high = low + block_cols
        partial_sum = jnp.dot(grad_value[:, low:high], w_value[:, low:high].T, preferred_element_type=jnp.float32)
        partial_sum = partial_sum + jnp.dot(grad_gate[:, low:high], w_gate[:, low:high].T, preferred_element_type=jnp.float32)
        summed = summed + partial_sum.astype(jnp.bfloat16).astype(jnp.float32)
    input_grad = summed.astype(jnp.bfloat16)
    loss_scale = 1.0 / jnp.sqrt(jnp.float32(TOKENS))
    value_wgrad = jnp.dot(block_input.T, grad_value, preferred_element_type=jnp.float32) * loss_scale
    gate_wgrad = jnp.dot(block_input.T, grad_gate, preferred_element_type=jnp.float32) * loss_scale
    proj_wgrad = jnp.dot(mixer_out.T, out_grad, preferred_element_type=jnp.float32) * loss_scale
    taps_grad = jnp.stack(taps_rows, axis=0) * loss_scale
    gain_grad = lax.optimization_barrier(jnp.sum(grad_act * normed, axis=0)) * loss_scale
    shift_grad = lax.optimization_barrier(jnp.sum(grad_act, axis=0)) * loss_scale
    return (input_grad, value_wgrad, gate_wgrad, proj_wgrad, taps_grad, gain_grad, shift_grad)
```

```python
import math

import jax
import jax.numpy as jnp
from jax import lax
from jax.sharding import PartitionSpec as P

EPS = 0.05
HALO = 32
bf16 = jnp.bfloat16
f32 = jnp.float32


def send(block, axis, target):
    devices = range(lax.axis_size(axis))
    route = [(i, target(i)) for i in devices if 0 <= target(i) < len(devices)]
    return lax.ppermute(block, axis, route)


def all_sum(block, axis):
    step = 1
    while step < lax.axis_size(axis):
        block = block + send(block, axis, lambda i, b=step: i ^ b)
        step *= 2
    return block


def radices(size):
    out = []
    for r in (2, 4):
        if size % r == 0 and size > 1:
            out.append(r)
            size //= r
    if size > 1:
        out.append(size)
    return out


def reduce_scatter(parts, rider=None):
    n = parts.shape[0]
    me = lax.axis_index("sp")
    stride = 1
    for r in radices(n):
        digit = (me // stride) % r
        m = parts.shape[0] // r
        view = parts.reshape((m, r) + parts.shape[1:])

        def pick(k):
            return lax.dynamic_index_in_dim(view, (digit + k) % r, 1, keepdims=False)

        acc = pick(0)
        cols = parts.shape[2]
        if rider is not None:
            high = rider.astype(bf16)
            low = (rider - high.astype(f32)).astype(bf16)
            pack = jnp.concatenate([high, low], axis=1)
            around = [pack]
        for k in range(1, r):
            message = pick(k).astype(bf16).reshape(-1, cols)
            if rider is not None:
                message = jnp.concatenate([message, pack], axis=0)
            got = send(
                message, "sp", lambda i, k=k, r=r, s=stride: i + (((i // s) % r + k) % r - (i // s) % r) * s
            )
            if rider is not None:
                around.append(got[m * parts.shape[1] :])
                got = got[: m * parts.shape[1]]
            acc = acc + got.reshape(acc.shape).astype(f32)
        if rider is not None:
            pile = jnp.stack(around).astype(f32)
            half = cols // 2
            pile = pile[:, :, :half] + pile[:, :, half:]
            order = (digit - jnp.arange(r)) % r
            total = jnp.take(pile, order[0], axis=0)
            for j in range(1, r):
                total = total + jnp.take(pile, order[j], axis=0)
            rider = total
        parts = acc
        stride *= r
    return parts[0], rider


def right_product(left, right):
    return lax.dot_general(left, right, (((1,), (1,)), ((), ())), preferred_element_type=f32)


def column_product(left, right):
    return lax.dot_general(left, right, (((0,), (0,)), ((), ())), preferred_element_type=f32)


def shards(block_input, out_grad, w_value, w_gate, conv_taps, norm_gain, norm_shift, w_proj):
    tok = block_input.shape[0]
    width = block_input.shape[1]
    taps = conv_taps.shape[0]
    ch = w_value.shape[1]
    n_tp = lax.axis_size("tp")
    n_sp = lax.axis_size("sp")
    channels = ch * n_tp
    loss_scale = 1.0 / math.sqrt(tok * n_sp)
    t_me = lax.axis_index("tp")
    own_cols = width // n_tp

    edge = jnp.concatenate([block_input[:HALO], block_input[tok - HALO :]], axis=0)
    edge_value = jnp.dot(edge, w_value, preferred_element_type=f32).astype(bf16)
    edge_gate = jnp.dot(edge, w_gate, preferred_element_type=f32).astype(bf16)
    edge_glu = (edge_value.astype(f32) * jax.nn.sigmoid(edge_gate.astype(f32))).astype(bf16)
    edge_mixed = right_product(out_grad[:HALO], w_proj)
    before = send(edge_glu[HALO:], "sp", lambda i: i + 1)
    after = send(
        jnp.concatenate([edge_glu[:HALO].astype(f32), edge_mixed], axis=0), "sp", lambda i: i - 1
    )

    value_proj = jnp.dot(block_input, w_value, preferred_element_type=f32).astype(bf16)
    gate_proj = jnp.dot(block_input, w_gate, preferred_element_type=f32).astype(bf16)
    gate_sigmoid = jax.nn.sigmoid(gate_proj.astype(f32))
    value_wide = value_proj.astype(f32)
    gated_input = (value_wide * gate_sigmoid).astype(bf16)
    grad_mixed = jnp.concatenate([right_product(out_grad, w_proj), after[HALO:]], axis=0)
    extended = jnp.concatenate([before.astype(f32), gated_input.astype(f32), after[:HALO]], axis=0)
    rows = tok + HALO
    filtered = jnp.zeros((rows, ch), f32)
    for k in range(taps):
        filtered = filtered + conv_taps[k] * extended[HALO - k : HALO - k + rows]
    stats = all_sum(
        jnp.stack([jnp.sum(filtered, axis=1), jnp.sum(filtered * filtered, axis=1)]), "tp"
    )
    row_mean = stats[0] / channels
    row_var = stats[1] / channels - row_mean * row_mean
    row_scale = lax.rsqrt(row_var + EPS)
    normed = (filtered - row_mean[:, None]) * row_scale[:, None]
    activated = normed * norm_gain + norm_shift
    act_sigmoid = jax.nn.sigmoid(activated)
    mixer_out = (activated * act_sigmoid)[:tok].astype(bf16)
    grad_act = grad_mixed * act_sigmoid * (1.0 + activated * (1.0 - act_sigmoid))
    grad_normed = grad_act * norm_gain
    back = all_sum(
        jnp.stack([jnp.sum(grad_normed, axis=1), jnp.sum(grad_normed * normed, axis=1)]), "tp"
    )
    proj_part = column_product(out_grad, mixer_out)
    proj_sum, _ = reduce_scatter(proj_part.reshape(n_sp, width // n_sp, ch))

    grad_filtered = row_scale[:, None] * (
        grad_normed - back[0][:, None] / channels - normed * (back[1][:, None] / channels)
    )
    gain_part = jnp.sum(grad_act[:tok] * normed[:tok], axis=0)
    shift_part = jnp.sum(grad_act[:tok], axis=0)
    grad_glu = jnp.zeros((tok, ch), f32)
    small_rows = []
    for k in range(taps):
        grad_glu = grad_glu + conv_taps[k] * grad_filtered[k : k + tok]
        small_rows.append(
            jnp.sum(grad_filtered[:tok] * extended[HALO - k : HALO - k + tok], axis=0)
        )
    pad = (-(taps + 2)) % 16
    small = jnp.stack(small_rows + [gain_part, shift_part] + [jnp.zeros_like(gain_part)] * pad)
    grad_value = (grad_glu * gate_sigmoid).astype(bf16)
    grad_gate = (grad_glu * value_wide * gate_sigmoid * (1.0 - gate_sigmoid)).astype(bf16)
    grad_both = jnp.concatenate([grad_value, grad_gate], axis=1)

    w_both = jnp.concatenate([w_value, w_gate], axis=1)
    weights = [lax.dynamic_slice_in_dim(w_both, t_me * own_cols, own_cols, 0)]
    for b in range(1, n_tp):
        weights.append(
            send(
                lax.dynamic_slice_in_dim(w_both, (t_me ^ b) * own_cols, own_cols, 0),
                "tp",
                lambda i, b=b: i ^ b,
            )
        )
    have = {0: grad_both}
    step = n_tp // 2
    while step:
        for key in list(have):
            have[key ^ step] = send(have[key], "tp", lambda i, b=step: i ^ b)
        step //= 2
    total = right_product(have[0], weights[0])
    for b in range(1, n_tp):
        total = total + right_product(have[b], weights[b])
    input_grad = total.astype(bf16)

    weight_part = column_product(block_input, grad_both)
    weight_sum, small_sum = reduce_scatter(
        weight_part.reshape(n_sp, width // n_sp, 2 * ch), small
    )
    return (
        input_grad,
        weight_sum[:, :ch] * loss_scale,
        weight_sum[:, ch:] * loss_scale,
        (proj_sum * loss_scale).T,
        small_sum[:taps] * loss_scale,
        small_sum[taps] * loss_scale,
        small_sum[taps + 1] * loss_scale,
    )


def solution(mesh):
    return jax.shard_map(
        shards,
        mesh=mesh,
        in_specs=(
            P("sp", None),
            P("sp", None),
            P(None, "tp"),
            P(None, "tp"),
            P(None, "tp"),
            P("tp"),
            P("tp"),
            P("tp", None),
        ),
        out_specs=(
            P("sp", "tp"),
            P("sp", "tp"),
            P("sp", "tp"),
            P("tp", "sp"),
            P(None, "tp"),
            P("tp"),
            P("tp"),
        ),
        check_vma=False,
    )
```

```python
import functools
import math

import jax
import jax.numpy as jnp
from jax import lax
from jax.experimental import pallas as pl
from jax.experimental.pallas import tpu as pltpu
from jax.sharding import PartitionSpec as P

EPS = 0.05
HALO = 32
LANE = 128
bf16 = jnp.bfloat16
f32 = jnp.float32
VMEM = pltpu.CompilerParams(vmem_limit_bytes=48 * 1024 * 1024)


def send(block, axis, target):
    devices = range(lax.axis_size(axis))
    route = [(i, target(i)) for i in devices if 0 <= target(i) < len(devices)]
    return lax.ppermute(block, axis, route)


def swap(block, axis, bit):
    return send(block, axis, lambda i: i ^ bit)


def all_sum(block, axis):
    step = 1
    while step < lax.axis_size(axis):
        block = block + swap(block, axis, step)
        step *= 2
    return block


def after_value(block, gate):
    return lax.optimization_barrier((block, gate))[0]


def radices(size):
    out = []
    for r in (2, 4):
        if size % r == 0 and size > 1:
            out.append(r)
            size //= r
    if size > 1:
        out.append(size)
    return out


def right_product(left, right):
    return lax.dot_general(left, right, (((1,), (1,)), ((), ())), preferred_element_type=f32)


def blocks_kernel(digit_ref, left_ref, right_ref, out_ref):
    out_ref[0] = jnp.dot(left_ref[...], right_ref[...], preferred_element_type=f32).astype(
        out_ref.dtype
    )


def grad_blocks(left, right, digit, radix, n, dtype):
    rows, tok = left.shape
    width = right.shape[1] // n
    count = n // radix
    if width % LANE:
        view = right.reshape(tok, count, radix, width)
        mine = lax.dynamic_index_in_dim(view, digit, 2, keepdims=False).reshape(tok, count * width)
        out = jnp.dot(left, mine, preferred_element_type=f32).astype(dtype)
        return out.reshape(rows, count, width).transpose(1, 0, 2)
    return pl.pallas_call(
        blocks_kernel,
        grid_spec=pltpu.PrefetchScalarGridSpec(
            num_scalar_prefetch=1,
            grid=(count,),
            in_specs=[
                pl.BlockSpec((rows, tok), lambda i, d: (0, 0)),
                pl.BlockSpec((tok, width), lambda i, d: (0, i * radix + d[0])),
            ],
            out_specs=pl.BlockSpec((1, rows, width), lambda i, d: (i, 0, 0)),
        ),
        out_shape=jax.ShapeDtypeStruct((count, rows, width), dtype),
        compiler_params=VMEM,
        cost_estimate=pl.CostEstimate(
            flops=2 * rows * tok * count * width,
            transcendentals=0,
            bytes_accessed=2 * tok * (rows + count * width) + 4 * rows * count * width,
        ),
        name="grad_blocks",
    )(digit.reshape(1), left, right)


def shift(k, radix, stride):
    def target(i):
        own = (i // stride) % radix
        return i + ((own + k) % radix - own) * stride

    return target


def digits_of(axis):
    me = lax.axis_index(axis)
    out = []
    stride = 1
    for r in radices(lax.axis_size(axis)):
        out.append((r, stride, (me // stride) % r))
        stride *= r
    return out


def reduce_blocks(make, axis):
    digits = digits_of(axis)
    first, _, digit = digits[0]
    outs = [make((digit + k) % first, first, bf16) for k in range(1, first)]
    got = [send(o, axis, shift(k + 1, first, 1)) for k, o in enumerate(outs)]
    own = make(digit, first, f32)
    for r, stride, digit in digits[1:]:
        m = own.shape[0] // r
        shape = (m, r) + own.shape[1:]

        def pick(k):
            part = lax.dynamic_index_in_dim(own.reshape(shape), (digit + k) % r, 1, keepdims=False)
            for g in got:
                part = part + lax.dynamic_index_in_dim(
                    g.reshape(shape), (digit + k) % r, 1, keepdims=False
                ).astype(f32)
            return part

        sent = [send(pick(k).astype(bf16), axis, shift(k, r, stride)) for k in range(1, r)]
        own = pick(0)
        got = sent
    for g in got:
        own = own + g.astype(f32)
    return own[0]


def project_kernel(x_ref, wv_ref, wg_ref, edge_ref, wp_ref, v_out, s_out, u_out, m_out):
    x = x_ref[...]
    v = jnp.dot(x, wv_ref[...], preferred_element_type=f32).astype(bf16)
    s = jnp.dot(x, wg_ref[...], preferred_element_type=f32).astype(bf16)
    v_out[...] = v
    s_out[...] = s
    u_out[...] = (v.astype(f32) * jax.nn.sigmoid(s.astype(f32))).astype(bf16)

    @pl.when(pl.program_id(0) == 0)
    def _():
        m_out[...] = right_product(edge_ref[...], wp_ref[...])


def project(x, wv, wg, g, wp, block):
    t, d = x.shape
    c = wv.shape[1]
    return pl.pallas_call(
        project_kernel,
        grid=(t // block,),
        in_specs=[
            pl.BlockSpec((block, d), lambda i: (i, 0)),
            pl.BlockSpec((d, c), lambda i: (0, 0)),
            pl.BlockSpec((d, c), lambda i: (0, 0)),
            pl.BlockSpec((HALO, d), lambda i: (0, 0)),
            pl.BlockSpec((c, d), lambda i: (0, 0)),
        ],
        out_specs=[pl.BlockSpec((block, c), lambda i: (i, 0))] * 3
        + [pl.BlockSpec((HALO, c), lambda i: (0, 0))],
        out_shape=[jax.ShapeDtypeStruct((t, c), bf16)] * 3 + [jax.ShapeDtypeStruct((HALO, c), f32)],
        compiler_params=VMEM,
        cost_estimate=pl.CostEstimate(
            flops=4 * t * d * c, transcendentals=t * c, bytes_accessed=2 * (t * d + 3 * d * c + 3 * t * c)
        ),
        name="project",
    )(x, wv, wg, g, wp)


def back_kernel(g_ref, w_ref, out_ref):
    out_ref[...] = right_product(g_ref[...], w_ref[...])


def back_project(g, w, block):
    t, d = g.shape
    c = w.shape[0]
    return pl.pallas_call(
        back_kernel,
        grid=(t // block,),
        in_specs=[pl.BlockSpec((block, d), lambda i: (i, 0)), pl.BlockSpec((c, d), lambda i: (0, 0))],
        out_specs=pl.BlockSpec((block, c), lambda i: (i, 0)),
        out_shape=jax.ShapeDtypeStruct((t, c), f32),
        compiler_params=VMEM,
        cost_estimate=pl.CostEstimate(
            flops=2 * t * d * c, transcendentals=0, bytes_accessed=2 * t * d + 2 * d * c + 4 * t * c
        ),
        name="back_project",
    )(g, w)


def chunk_of(rows, most):
    return max(c for c in range(16, most + 1, 16) if rows % c == 0)


def fill_extended(ext_ref, before, glu, after, tok):
    ext_ref[pl.ds(0, HALO), :] = before.astype(f32)
    ext_ref[pl.ds(HALO, tok), :] = glu.astype(f32)
    ext_ref[pl.ds(HALO + tok, HALO), :] = after


def tap_rows(taps_ref, taps):
    return [jnp.broadcast_to(taps_ref[pl.ds(k, 1), :], (8, LANE)) for k in range(taps)]


def conv_kernel(before_ref, glu_ref, after_ref, taps_ref, out_ref, ext_ref):
    tok = glu_ref.shape[0]
    rows = tok + HALO
    taps = taps_ref.shape[0]
    chunk = chunk_of(rows, 96)
    fill_extended(ext_ref, before_ref[...], glu_ref[...], after_ref[...], tok)
    weights = tap_rows(taps_ref, taps)

    def step(i, carry):
        base = pl.multiple_of(i * chunk, chunk)
        x = ext_ref[pl.ds(base, chunk + HALO), :]
        acc = [None] * (chunk // 8)
        for r in range(8):
            moved = x if r == 0 else pltpu.roll(x, r, 0)
            for k in range(r, taps, 8):
                for j in range(chunk // 8):
                    low = HALO + 8 * j - (k - r)
                    part = weights[k] * moved[low : low + 8]
                    acc[j] = part if acc[j] is None else acc[j] + part
        for j in range(chunk // 8):
            out_ref[pl.ds(base + 8 * j, 8), :] = acc[j]
        return carry

    lax.fori_loop(0, rows // chunk, step, 0)


def convolve(before, glu, after, conv_taps):
    tok, ch = glu.shape
    taps = conv_taps.shape[0]
    column = lambda i: (0, i)
    return pl.pallas_call(
        conv_kernel,
        grid=(ch // LANE,),
        in_specs=[
            pl.BlockSpec((HALO, LANE), column),
            pl.BlockSpec((tok, LANE), column),
            pl.BlockSpec((HALO, LANE), column),
            pl.BlockSpec((taps, LANE), column),
        ],
        out_specs=pl.BlockSpec((tok + HALO, LANE), column),
        out_shape=jax.ShapeDtypeStruct((tok + HALO, ch), f32),
        scratch_shapes=[pltpu.VMEM((tok + 2 * HALO, LANE), f32)],
        compiler_params=VMEM,
        cost_estimate=pl.CostEstimate(
            flops=20 * taps * tok * ch, transcendentals=0, bytes_accessed=6 * tok * ch
        ),
        name="convolve",
    )(before, glu, after, conv_taps)


def back_conv_kernel(
    grad_ref, before_ref, glu_ref, after_ref, v_ref, s_ref, taps_ref, out_ref, turned_ref, small_ref, ext_ref
):
    tok = glu_ref.shape[0]
    taps = taps_ref.shape[0]
    fill_extended(ext_ref, before_ref[...], glu_ref[...], after_ref[...], tok)
    weights = tap_rows(taps_ref, taps)
    chunk = chunk_of(tok, 64)

    def spread(i, carry):
        base = pl.multiple_of(i * chunk, chunk)
        x = grad_ref[pl.ds(base, chunk + HALO), :]
        acc = [None] * (chunk // 8)
        for r in range(8):
            moved = x if r == 0 else pltpu.roll(x, chunk + HALO - r, 0)
            for k in range(r, taps, 8):
                for j in range(chunk // 8):
                    low = 8 * j + k - r
                    part = weights[k] * moved[low : low + 8]
                    acc[j] = part if acc[j] is None else acc[j] + part
        glu = jnp.concatenate(acc, axis=0)
        v = v_ref[pl.ds(base, chunk), :].astype(f32)
        s = jax.nn.sigmoid(s_ref[pl.ds(base, chunk), :].astype(f32))
        through = glu * s
        out_ref[pl.ds(base, chunk), pl.ds(0, LANE)] = through.astype(bf16)
        out_ref[pl.ds(base, chunk), pl.ds(LANE, LANE)] = (through * v * (1.0 - s)).astype(bf16)
        return carry

    lax.fori_loop(0, tok // chunk, spread, 0)
    for i in range(0, tok, LANE):
        turned_ref[:, pl.ds(i, LANE)] = out_ref[pl.ds(i, LANE), :].T

    width = chunk_of(tok, 32)

    def gather(i, sums):
        base = pl.multiple_of(i * width, width)
        g = grad_ref[pl.ds(base, width), :]
        x = ext_ref[pl.ds(base, width + HALO), :]
        sums = list(sums)
        for r in range(8):
            moved = x if r == 0 else pltpu.roll(x, r, 0)
            for k in range(r, taps, 8):
                for j in range(width // 8):
                    low = HALO + 8 * j - (k - r)
                    sums[k] = sums[k] + g[8 * j : 8 * j + 8] * moved[low : low + 8]
        return tuple(sums)

    zero = jnp.zeros((8, LANE), f32)
    sums = lax.fori_loop(0, tok // width, gather, (zero,) * taps)
    for k in range(taps):
        small_ref[pl.ds(k, 1), :] = jnp.sum(sums[k], axis=0, keepdims=True)
    for k in range(taps, small_ref.shape[0]):
        small_ref[pl.ds(k, 1), :] = jnp.zeros((1, LANE), f32)


def back_convolve(grad, before, glu, after, v, s, conv_taps, h):
    tok, ch = glu.shape
    taps = conv_taps.shape[0]
    column = lambda i: (0, h)
    first = lambda i: (0, 0)
    kept = -(-taps // 8) * 8
    return pl.pallas_call(
        back_conv_kernel,
        grid=(1,),
        in_specs=[
            pl.BlockSpec((tok + HALO, LANE), column),
            pl.BlockSpec((HALO, LANE), column),
            pl.BlockSpec((tok, LANE), column),
            pl.BlockSpec((HALO, LANE), column),
            pl.BlockSpec((tok, LANE), column),
            pl.BlockSpec((tok, LANE), column),
            pl.BlockSpec((taps, LANE), column),
        ],
        out_specs=[
            pl.BlockSpec((tok, 2 * LANE), first),
            pl.BlockSpec((2 * LANE, tok), first),
            pl.BlockSpec((kept, LANE), first),
        ],
        out_shape=[
            jax.ShapeDtypeStruct((tok, 2 * LANE), bf16),
            jax.ShapeDtypeStruct((2 * LANE, tok), bf16),
            jax.ShapeDtypeStruct((kept, LANE), f32),
        ],
        scratch_shapes=[pltpu.VMEM((tok + 2 * HALO, LANE), f32)],
        compiler_params=VMEM,
        cost_estimate=pl.CostEstimate(
            flops=40 * taps * tok * LANE, transcendentals=0, bytes_accessed=16 * tok * LANE
        ),
        name="back_convolve",
    )(grad, before, glu, after, v, s, conv_taps)


def input_kernel(digit_ref, *refs, halves):
    out_ref = refs[-1]
    value_ref, gate_ref = refs[halves : halves + 2]
    total = None
    for h in range(halves):
        cols = pl.ds(h * LANE, LANE)
        weight = jnp.concatenate([value_ref[:, cols], gate_ref[:, cols]], axis=1)
        part = right_product(refs[h][...], weight)
        total = part if total is None else total + part
    out_ref[0] = total.astype(bf16)


def input_blocks(grads, w_value, w_gate, digit, radix, n):
    halves = len(grads)
    t = grads[0].shape[0]
    d, c = w_value.shape
    width = d // n
    count = n // radix
    return pl.pallas_call(
        functools.partial(input_kernel, halves=halves),
        grid_spec=pltpu.PrefetchScalarGridSpec(
            num_scalar_prefetch=1,
            grid=(count,),
            in_specs=[pl.BlockSpec((t, 2 * LANE), lambda i, d: (0, 0))] * halves
            + [pl.BlockSpec((width, c), lambda i, d: (i * radix + d[0], 0))] * 2,
            out_specs=pl.BlockSpec((1, t, width), lambda i, d: (i, 0, 0)),
        ),
        out_shape=jax.ShapeDtypeStruct((count, t, width), bf16),
        compiler_params=VMEM,
        cost_estimate=pl.CostEstimate(
            flops=4 * t * c * count * width,
            transcendentals=0,
            bytes_accessed=2 * (2 * t * c + 2 * count * width * c + count * t * width),
        ),
        name="input_blocks",
    )(digit.reshape(1), *grads, w_value, w_gate)


def shards(block_input, out_grad, w_value, w_gate, conv_taps, norm_gain, norm_shift, w_proj):
    tok, width = block_input.shape
    taps = conv_taps.shape[0]
    ch = w_value.shape[1]
    n_tp = lax.axis_size("tp")
    n_sp = lax.axis_size("sp")
    channels = ch * n_tp
    loss_scale = 1.0 / math.sqrt(tok * n_sp)
    value_proj, gate_proj, gated_input, edge_mixed = project(
        block_input, w_value, w_gate, out_grad, w_proj, min(512, tok)
    )
    before = send(gated_input[tok - HALO :], "sp", lambda i: i + 1)
    after = send(
        jnp.concatenate([gated_input[:HALO].astype(f32), edge_mixed], axis=0), "sp", lambda i: i - 1
    )
    own_mixed = back_project(out_grad, w_proj, min(512, tok))
    rows = tok + HALO
    filtered = convolve(before, gated_input, after, conv_taps)
    stats = all_sum(
        jnp.stack([jnp.sum(filtered, axis=1), jnp.sum(filtered * filtered, axis=1)]), "tp"
    )
    row_mean = stats[0] / channels
    row_var = stats[1] / channels - row_mean * row_mean
    row_scale = lax.rsqrt(row_var + EPS)
    normed = (filtered - row_mean[:, None]) * row_scale[:, None]
    activated = normed * norm_gain + norm_shift
    act_sigmoid = jax.nn.sigmoid(activated)
    mixer_out = (activated * act_sigmoid)[:tok].astype(bf16)
    grad_mixed = jnp.concatenate([own_mixed, after[HALO:]], axis=0)
    grad_act = grad_mixed * act_sigmoid * (1.0 + activated * (1.0 - act_sigmoid))
    grad_normed = grad_act * norm_gain
    back = all_sum(
        jnp.stack([jnp.sum(grad_normed, axis=1), jnp.sum(grad_normed * normed, axis=1)]), "tp"
    )
    turned = mixer_out.T
    proj_sum = reduce_blocks(
        lambda digit, radix, dtype: grad_blocks(turned, out_grad, digit, radix, n_sp, dtype), "sp"
    )
    grad_filtered = row_scale[:, None] * (
        grad_normed - back[0][:, None] / channels - normed * (back[1][:, None] / channels)
    )
    gain_part = jnp.sum(grad_act[:tok] * normed[:tok], axis=0)
    shift_part = jnp.sum(grad_act[:tok], axis=0)

    halves = ch // LANE
    grads = []
    sums = []
    small = []
    for h in range(halves):
        grad, turn, tap_sums = back_convolve(
            grad_filtered, before, gated_input, after, value_proj, gate_proj, conv_taps, h
        )
        grads.append(grad)
        small.append(tap_sums)
        sums.append(
            reduce_blocks(
                lambda digit, radix, dtype, turn=turn: grad_blocks(
                    turn, block_input, digit, radix, n_sp, dtype
                ),
                "sp",
            )
        )
    kept = small[0].shape[0]
    edge = jnp.concatenate([jnp.stack([gain_part, shift_part]), jnp.zeros((6, ch), f32)], axis=0)
    small_sum = all_sum(jnp.concatenate([jnp.concatenate(small, axis=1), edge], axis=0), "sp")
    input_sum = reduce_blocks(
        lambda digit, radix, dtype: input_blocks(grads, w_value, w_gate, digit, radix, n_tp), "tp"
    )
    value_sum = jnp.concatenate([s[:LANE] for s in sums], axis=0)
    gate_sum = jnp.concatenate([s[LANE:] for s in sums], axis=0)
    return (
        input_sum.astype(bf16),
        value_sum.T * loss_scale,
        gate_sum.T * loss_scale,
        proj_sum * loss_scale,
        small_sum[:taps] * loss_scale,
        small_sum[kept] * loss_scale,
        small_sum[kept + 1] * loss_scale,
    )


def solution(mesh):
    return jax.shard_map(
        shards,
        mesh=mesh,
        in_specs=(
            P("sp", None),
            P("sp", None),
            P(None, "tp"),
            P(None, "tp"),
            P(None, "tp"),
            P("tp"),
            P("tp"),
            P("tp", None),
        ),
        out_specs=(
            P("sp", "tp"),
            P("sp", "tp"),
            P("sp", "tp"),
            P("tp", "sp"),
            P(None, "tp"),
            P("tp"),
            P("tp"),
        ),
        check_vma=False,
    )
```

```python
import functools
import math

import jax
import jax.numpy as jnp
from jax import lax
from jax.experimental import pallas as pl
from jax.experimental.pallas import tpu as pltpu
from jax.sharding import PartitionSpec as P


EPS = 0.05
HALO = 32
LANE = 128
bf16 = jnp.bfloat16
f32 = jnp.float32


VMEM_SPEC = pl.BlockSpec(memory_space=pltpu.VMEM)
SMEM_SPEC = pl.BlockSpec(memory_space=pltpu.SMEM)


def limit(mib):
    return pltpu.CompilerParams(vmem_limit_bytes=mib * 1024 * 1024)


def send(block, axis, target):
    devices = range(lax.axis_size(axis))
    route = [(i, target(i)) for i in devices if 0 <= target(i) < len(devices)]
    return lax.ppermute(block, axis, route)


def all_sum(block, axis):
    step = 1
    while step < lax.axis_size(axis):
        block = block + send(block, axis, lambda i, b=step: i ^ b)
        step *= 2
    return block


def in_hbm(block):
    return pltpu.with_memory_space_constraint(block, pltpu.HBM)


def radices(size):
    out = []
    for r in (2, 4):
        if size % r == 0 and size > 1:
            out.append(r)
            size //= r
    if size > 1:
        out.append(size)
    return out


def right_product(left, right):
    return lax.dot_general(left, right, (((1,), (1,)), ((), ())), preferred_element_type=f32)


def blocks_kernel(ids_ref, left_ref, right_ref, *refs, gives):
    rider = refs[: -gives - 1]
    outs = refs[-gives - 1 : -1]
    own = refs[-1]
    rows = left_ref.shape[0]
    width = own.shape[2]
    count = own.shape[0]
    left = left_ref[...]

    def block(i):
        start = pl.multiple_of(ids_ref[i] * width, LANE)
        return jnp.dot(left, right_ref[:, pl.ds(start, width)], preferred_element_type=f32)

    for i, out in enumerate(outs):
        for j in range(count):
            out[pl.ds(j * rows, rows), :] = block(i * count + j).astype(bf16)
        for m, extra in enumerate(rider):
            size = extra.shape[0]
            out[pl.ds(count * rows + m * size, size), :] = extra[...]
    for j in range(count):
        own[j] = block(len(outs) * count + j)


def grad_blocks(left, right, ids, n, rider):
    rows, tok = left.shape
    width = right.shape[1] // n
    count = ids[0].shape[0]
    gives = len(ids) - 1
    extra = sum(a.shape[0] for a in rider)
    if width % LANE:
        full = jnp.dot(left, right, preferred_element_type=f32).reshape(rows, n, width)
        full = full.transpose(1, 0, 2)
        outs = [jnp.take(full, some, axis=0) for some in ids]
        below = [a.reshape(-1, width) for a in rider]
        return [
            jnp.concatenate([o.astype(bf16).reshape(-1, width)] + below, axis=0) for o in outs[:-1]
        ] + outs[-1:]
    return pl.pallas_call(
        functools.partial(blocks_kernel, gives=gives),
        in_specs=[SMEM_SPEC] + [VMEM_SPEC] * (2 + len(rider)),
        out_specs=[VMEM_SPEC] * (gives + 1),
        out_shape=[jax.ShapeDtypeStruct((count * rows + extra, width), bf16)] * gives
        + [jax.ShapeDtypeStruct((count, rows, width), f32)],
        compiler_params=limit(10),
        cost_estimate=pl.CostEstimate(
            flops=2 * rows * tok * count * width * len(ids),
            transcendentals=0,
            bytes_accessed=2 * tok * (rows + count * width * len(ids)) + 4 * rows * count * width * len(ids),
        ),
        name="grad_blocks",
    )(jnp.concatenate(ids).astype(jnp.int32), left, right, *rider)


def shift(k, radix, stride):
    def target(i):
        own = (i // stride) % radix
        return i + ((own + k) % radix - own) * stride

    return target


def two_parts(block):
    high = block.astype(bf16)
    return [high, (block - high.astype(f32)).astype(bf16)]


def reduce_blocks(left, right, small=None, last_first=False):
    n = lax.axis_size("sp")
    me = lax.axis_index("sp")
    stages = []
    stride = 1
    for r in radices(n):
        stages.append((r, stride, (me // stride) % r))
        stride *= r
    if last_first:
        stages.reverse()
    base = jnp.zeros((1,), jnp.int32)
    for r, stride, _ in stages[1:]:
        base = (base[:, None] + stride * jnp.arange(r)[None]).reshape(-1)
    rest = tuple(r for r, _, _ in stages[1:])
    r, stride, digit = stages[0]
    rows = left.shape[0]
    width = right.shape[1] // n

    def ids(k):
        return base + (digit + k) % r * stride

    def whole(parts):
        return (parts[0].astype(f32) + parts[1].astype(f32)).reshape(small.shape)

    def split(message, above):
        rider = message[above:]
        half = rider.shape[0] // 2
        return message[:above], whole([rider[:half], rider[half:]])

    def total(own, got, digit, r):
        if r == 2:
            return own + got[0]
        pile = jnp.stack([own] + got)
        order = [
            lax.dynamic_index_in_dim(pile, (digit - j) % r, 0, keepdims=False) for j in range(r)
        ]
        return sum(order[1:], order[0])

    rider = [] if small is None else two_parts(small)
    *outs, own = grad_blocks(left, right, [ids(k) for k in range(1, r)] + [ids(0)], n, rider)
    got = [send(o, "sp", shift(k + 1, r, stride)) for k, o in enumerate(outs)]
    if small is not None:
        pairs = [split(g, base.shape[0] * rows) for g in got]
        got = [p[0] for p in pairs]
        small = total(whole(rider), [p[1] for p in pairs], digit, r)
    parts = [own.reshape(rest + (rows, width))] + [g.reshape(rest + (rows, width)) for g in got]
    for r, stride, digit in stages[1:]:

        def pick(k):
            return sum(
                lax.dynamic_index_in_dim(p, (digit + k) % r, 0, keepdims=False).astype(f32) for p in parts
            )

        sent = [pick(k).astype(bf16) for k in range(1, r)]
        shape = sent[0].shape
        if small is not None:
            rider = [a.reshape(-1, width) for a in two_parts(small)]
            sent = [jnp.concatenate([x.reshape(-1, width)] + rider, axis=0) for x in sent]
        got = [send(x, "sp", shift(k + 1, r, stride)) for k, x in enumerate(sent)]
        if small is not None:
            pairs = [split(g, g.shape[0] - 2 * rider[0].shape[0]) for g in got]
            got = [p[0].reshape(shape) for p in pairs]
            small = total(whole(rider), [p[1] for p in pairs], digit, r)
        parts = [pick(0)] + got
    return parts, small


def project_kernel(
    x_hbm, wv_hbm, wg_hbm, g_hbm, wp_hbm, v_out, s_out, u_out, m_out, x_buf, g_buf, wv_buf, wg_buf, wp_buf, sems
):
    count, block, _ = x_buf.shape

    def copies(at, hbm, buf):
        return [
            pltpu.make_async_copy(hbm.at[pl.ds(k * block, block), :], buf.at[k], sems.at[at, k])
            for k in range(count)
        ]

    weights = [
        pltpu.make_async_copy(hbm, buf, sems.at[2, k])
        for k, (hbm, buf) in enumerate(((wv_hbm, wv_buf), (wg_hbm, wg_buf), (wp_hbm, wp_buf)))
    ]
    inputs = copies(0, x_hbm, x_buf)
    grads = copies(1, g_hbm, g_buf)
    for copy in weights[:2] + inputs + weights[2:] + grads:
        copy.start()
    weights[0].wait()
    weights[1].wait()
    for k in range(count):
        inputs[k].wait()
        rows = pl.ds(k * block, block)
        v = jnp.dot(x_buf[k], wv_buf[...], preferred_element_type=f32).astype(bf16)
        s = jnp.dot(x_buf[k], wg_buf[...], preferred_element_type=f32).astype(bf16)
        v_out[rows, :] = v
        s_out[rows, :] = s
        u_out[rows, :] = (v.astype(f32) * jax.nn.sigmoid(s.astype(f32))).astype(bf16)
    weights[2].wait()
    for k in range(count):
        grads[k].wait()
        m_out[pl.ds(k * block, block), :] = right_product(g_buf[k], wp_buf[...])


def project(x, wv, wg, g, wp, count):
    t, d = x.shape
    c = wv.shape[1]
    hbm = pl.BlockSpec(memory_space=pl.ANY)
    return pl.pallas_call(
        project_kernel,
        in_specs=[hbm] * 5,
        out_specs=[VMEM_SPEC] * 4,
        out_shape=[jax.ShapeDtypeStruct((t, c), bf16)] * 3 + [jax.ShapeDtypeStruct((t, c), f32)],
        scratch_shapes=[
            pltpu.VMEM((count, t // count, d), bf16),
            pltpu.VMEM((count, t // count, d), bf16),
            pltpu.VMEM((d, c), bf16),
            pltpu.VMEM((d, c), bf16),
            pltpu.VMEM((c, d), bf16),
            pltpu.SemaphoreType.DMA((3, max(3, count))),
        ],
        compiler_params=limit(20),
        cost_estimate=pl.CostEstimate(
            flops=6 * t * d * c, transcendentals=t * c, bytes_accessed=2 * (2 * t * d + 3 * d * c + 5 * t * c)
        ),
        name="project",
    )(*(in_hbm(a) for a in (x, wv, wg, g, wp)))


def chunk_of(rows, most):
    return max(c for c in range(16, most + 1, 16) if rows % c == 0)


def fill_extended(ext_ref, before, glu, after, tok):
    ext_ref[pl.ds(0, HALO), :] = before.astype(f32)
    ext_ref[pl.ds(HALO, tok), :] = glu.astype(f32)
    ext_ref[pl.ds(HALO + tok, HALO), :] = after


def tap_rows(taps_ref, taps):
    return [jnp.broadcast_to(taps_ref[pl.ds(k, 1), :], (8, LANE)) for k in range(taps)]


def conv_rows(ext_ref, weights, base, chunk):
    x = ext_ref[pl.ds(base, chunk + HALO), :]
    acc = [None] * (chunk // 8)
    for r in range(8):
        moved = x if r == 0 else pltpu.roll(x, r, 0)
        for k in range(r, len(weights), 8):
            for j in range(chunk // 8):
                low = HALO + 8 * j - (k - r)
                part = weights[k] * moved[low : low + 8]
                acc[j] = part if acc[j] is None else acc[j] + part
    return acc


def conv_kernel(glu_ref, taps_ref, out_ref, wide_ref):
    tok = glu_ref.shape[0]
    rows = tok - HALO
    chunk = chunk_of(rows, 96)
    wide_ref[...] = glu_ref[...].astype(f32)
    weights = tap_rows(taps_ref, taps_ref.shape[0])

    def step(i, carry):
        base = pl.multiple_of(i * chunk, chunk)
        for j, part in enumerate(conv_rows(wide_ref, weights, base, chunk)):
            out_ref[pl.ds(base + HALO + 8 * j, 8), :] = part
        return carry

    lax.fori_loop(0, rows // chunk, step, 0)


def convolve(glu, conv_taps):
    tok, ch = glu.shape
    taps = conv_taps.shape[0]
    column = lambda i: (0, i)
    return pl.pallas_call(
        conv_kernel,
        grid=(ch // LANE,),
        in_specs=[pl.BlockSpec((tok, LANE), column), pl.BlockSpec((taps, LANE), column)],
        out_specs=pl.BlockSpec((tok + HALO, LANE), column),
        out_shape=jax.ShapeDtypeStruct((tok + HALO, ch), f32),
        scratch_shapes=[pltpu.VMEM((tok, LANE), f32)],
        compiler_params=limit(6),
        cost_estimate=pl.CostEstimate(
            flops=20 * taps * tok * ch, transcendentals=0, bytes_accessed=6 * tok * ch
        ),
        name="convolve",
    )(glu, conv_taps)


def ends_kernel(before_ref, head_ref, tail_ref, after_ref, taps_ref, main_ref, out_ref, ext_ref):
    ch = head_ref.shape[1]
    rows = main_ref.shape[0]
    for h in range(ch // LANE):
        cols = pl.ds(h * LANE, LANE)
        weights = [jnp.broadcast_to(taps_ref[pl.ds(k, 1), cols], (8, LANE)) for k in range(taps_ref.shape[0])]
        for m, (first, second) in enumerate(((before_ref, head_ref), (tail_ref, after_ref))):
            ext_ref[pl.ds(0, HALO), :] = first[:, cols].astype(f32)
            ext_ref[pl.ds(HALO, HALO), :] = second[pl.ds(0, HALO), cols].astype(f32)
            for j, part in enumerate(conv_rows(ext_ref, weights, 0, HALO)):
                out_ref[pl.ds(m * (rows - HALO) + 8 * j, 8), cols] = part


def convolve_ends(main, before, glu, after, conv_taps):
    return pl.pallas_call(
        ends_kernel,
        in_specs=[VMEM_SPEC] * 6,
        out_specs=VMEM_SPEC,
        out_shape=jax.ShapeDtypeStruct(main.shape, f32),
        input_output_aliases={5: 0},
        scratch_shapes=[pltpu.VMEM((2 * HALO, LANE), f32)],
        compiler_params=limit(4),
        cost_estimate=pl.CostEstimate(
            flops=80 * conv_taps.size * HALO, transcendentals=0, bytes_accessed=16 * HALO * main.shape[1]
        ),
        name="convolve_ends",
    )(before, glu[:HALO], glu[glu.shape[0] - HALO :], after, conv_taps, main)


def row_sums(first, second):
    pair = jnp.stack([jnp.sum(first, axis=1), jnp.sum(second, axis=1)])
    return jnp.pad(pair, ((0, 0), (0, -pair.shape[1] % LANE)))


def as_columns(rows):
    return jnp.pad(jnp.stack(rows), ((0, 8 - len(rows)), (0, 0)))


def act_kernel(
    filtered_ref, stats_ref, mixed_ref, edge_ref, gain_ref, shift_ref,
    normed_ref, grad_ref, turned_ref, sums_ref, col_ref, out_ref,
):
    ch = filtered_ref.shape[1]
    tok = mixed_ref.shape[0]
    col_ref[...] = stats_ref[...].T
    chunk = chunk_of(tok, 64)

    def some_rows(base, count, mixed, own):
        here = pl.ds(base, count)
        mean = jnp.broadcast_to(col_ref[here, pl.ds(0, 1)], (count, LANE))
        scale = jnp.broadcast_to(col_ref[here, pl.ds(1, 1)], (count, LANE))
        sums = []
        for h in range(ch // LANE):
            cols = pl.ds(h * LANE, LANE)
            normed = (filtered_ref[here, cols] - mean) * scale
            gain = gain_ref[:, cols]
            active = normed * gain + shift_ref[:, cols]
            s = jax.nn.sigmoid(active)
            act = mixed[:, h * LANE : (h + 1) * LANE] * s * (1.0 + active * (1.0 - s))
            normed_ref[here, cols] = normed
            grad_ref[here, cols] = act * gain
            if own:
                out_ref[here, cols] = (active * s).astype(bf16)
                sums.append(fold(act * normed))
                sums.append(fold(act))
        return sums

    def fold(x):
        total = x[0:8]
        for j in range(8, x.shape[0], 8):
            total = total + x[j : j + 8]
        return total

    def step(i, sums):
        base = pl.multiple_of(i * chunk, chunk)
        more = some_rows(base, chunk, mixed_ref[pl.ds(base, chunk), :], True)
        return tuple(a + b for a, b in zip(sums, more))

    zero = jnp.zeros((8, LANE), f32)
    sums = lax.fori_loop(0, tok // chunk, step, (zero,) * (2 * (ch // LANE)))
    some_rows(tok, HALO, edge_ref[...], False)
    sums_ref[...] = jnp.zeros_like(sums_ref)
    for h in range(ch // LANE):
        for m in range(2):
            sums_ref[pl.ds(m, 1), pl.ds(h * LANE, LANE)] = jnp.sum(sums[2 * h + m], axis=0, keepdims=True)
    for i in range(0, tok, LANE):
        turned_ref[:, pl.ds(i, LANE)] = out_ref[pl.ds(i, LANE), :].T


def activate(filtered, stats, mixed, after, gain, shift_row):
    rows, ch = filtered.shape
    tok = mixed.shape[0]
    wide = stats.shape[1]
    whole = lambda i: (0, 0)
    return pl.pallas_call(
        act_kernel,
        grid=(1,),
        in_specs=[
            pl.BlockSpec((rows, ch), whole),
            pl.BlockSpec((8, wide), whole),
            pl.BlockSpec((tok, ch), whole),
            pl.BlockSpec((HALO, ch), lambda i: (1, 0)),
            pl.BlockSpec((1, ch), whole),
            pl.BlockSpec((1, ch), whole),
        ],
        out_specs=[
            pl.BlockSpec((rows, ch), whole),
            pl.BlockSpec((rows, ch), whole),
            pl.BlockSpec((ch, tok), whole),
            pl.BlockSpec((16, ch), whole),
        ],
        out_shape=[
            jax.ShapeDtypeStruct((rows, ch), f32),
            jax.ShapeDtypeStruct((rows, ch), f32),
            jax.ShapeDtypeStruct((ch, tok), bf16),
            jax.ShapeDtypeStruct((16, ch), f32),
        ],
        scratch_shapes=[pltpu.VMEM((wide, 8), f32), pltpu.VMEM((tok, ch), bf16)],
        compiler_params=limit(12),
        cost_estimate=pl.CostEstimate(
            flops=200 * tok * ch, transcendentals=2 * tok * ch, bytes_accessed=18 * tok * ch
        ),
        name="activate",
    )(filtered, stats, mixed, after, gain, shift_row)


def back_conv_kernel(
    normed_ref, gn_ref, stats_ref, before_ref, glu_ref, after_ref, v_ref, s_ref, taps_ref,
    out_ref, turned_ref, small_ref, ext_ref, grad_ref, col_ref,
):
    tok = glu_ref.shape[0]
    rows = tok + HALO
    taps = taps_ref.shape[0]
    col_ref[...] = stats_ref[...].T
    fill_extended(ext_ref, before_ref[...], glu_ref[...], after_ref[...], tok)
    part_rows = chunk_of(rows, 96)

    def filtered_grad(i, carry):
        here = pl.ds(pl.multiple_of(i * part_rows, part_rows), part_rows)
        scale, first, second = (
            jnp.broadcast_to(col_ref[here, pl.ds(m, 1)], (part_rows, LANE)) for m in range(3)
        )
        grad_ref[here, :] = scale * (gn_ref[here, :] - first - normed_ref[here, :] * second)
        return carry

    lax.fori_loop(0, rows // part_rows, filtered_grad, 0)
    weights = tap_rows(taps_ref, taps)
    chunk = chunk_of(tok, 64)

    def spread(i, carry):
        base = pl.multiple_of(i * chunk, chunk)
        x = grad_ref[pl.ds(base, chunk + HALO), :]
        acc = [None] * (chunk // 8)
        for r in range(8):
            moved = x if r == 0 else pltpu.roll(x, chunk + HALO - r, 0)
            for k in range(r, taps, 8):
                for j in range(chunk // 8):
                    low = 8 * j + k - r
                    part = weights[k] * moved[low : low + 8]
                    acc[j] = part if acc[j] is None else acc[j] + part
        glu = jnp.concatenate(acc, axis=0)
        v = v_ref[pl.ds(base, chunk), :].astype(f32)
        s = jax.nn.sigmoid(s_ref[pl.ds(base, chunk), :].astype(f32))
        through = glu * s
        out_ref[pl.ds(base, chunk), pl.ds(0, LANE)] = through.astype(bf16)
        out_ref[pl.ds(base, chunk), pl.ds(LANE, LANE)] = (through * v * (1.0 - s)).astype(bf16)
        return carry

    lax.fori_loop(0, tok // chunk, spread, 0)
    for i in range(0, tok, LANE):
        turned_ref[:, pl.ds(i, LANE)] = out_ref[pl.ds(i, LANE), :].T

    width = chunk_of(tok, 32)

    def gather(i, sums):
        base = pl.multiple_of(i * width, width)
        g = grad_ref[pl.ds(base, width), :]
        x = ext_ref[pl.ds(base, width + HALO), :]
        sums = list(sums)
        for r in range(8):
            moved = x if r == 0 else pltpu.roll(x, r, 0)
            for k in range(r, taps, 8):
                for j in range(width // 8):
                    low = HALO + 8 * j - (k - r)
                    sums[k] = sums[k] + g[8 * j : 8 * j + 8] * moved[low : low + 8]
        return tuple(sums)

    zero = jnp.zeros((8, LANE), f32)
    sums = lax.fori_loop(0, tok // width, gather, (zero,) * taps)
    for k in range(taps):
        small_ref[pl.ds(k, 1), :] = jnp.sum(sums[k], axis=0, keepdims=True)
    for k in range(taps, small_ref.shape[0]):
        small_ref[pl.ds(k, 1), :] = jnp.zeros((1, LANE), f32)


def back_convolve(normed, gn, stats, before, glu, after, v, s, conv_taps, h):
    tok, _ = glu.shape
    taps = conv_taps.shape[0]
    wide = stats.shape[1]
    column = lambda i: (0, h)
    first = lambda i: (0, 0)
    kept = -(-taps // 8) * 8
    return pl.pallas_call(
        back_conv_kernel,
        grid=(1,),
        in_specs=[
            pl.BlockSpec((tok + HALO, LANE), column),
            pl.BlockSpec((tok + HALO, LANE), column),
            pl.BlockSpec((8, wide), first),
            pl.BlockSpec((HALO, LANE), column),
            pl.BlockSpec((tok, LANE), column),
            pl.BlockSpec((HALO, LANE), column),
            pl.BlockSpec((tok, LANE), column),
            pl.BlockSpec((tok, LANE), column),
            pl.BlockSpec((taps, LANE), column),
        ],
        out_specs=[
            pl.BlockSpec((tok, 2 * LANE), first),
            pl.BlockSpec((2 * LANE, tok), first),
            pl.BlockSpec((kept, LANE), first),
        ],
        out_shape=[
            jax.ShapeDtypeStruct((tok, 2 * LANE), bf16),
            jax.ShapeDtypeStruct((2 * LANE, tok), bf16),
            jax.ShapeDtypeStruct((kept, LANE), f32),
        ],
        scratch_shapes=[
            pltpu.VMEM((tok + 2 * HALO, LANE), f32),
            pltpu.VMEM((tok + HALO, LANE), f32),
            pltpu.VMEM((wide, 8), f32),
        ],
        compiler_params=limit(12),
        cost_estimate=pl.CostEstimate(
            flops=40 * taps * tok * LANE, transcendentals=0, bytes_accessed=16 * tok * LANE
        ),
        name="back_convolve",
    )(normed, gn, stats, before, glu, after, v, s, conv_taps)


def input_kernel(index_ref, *refs, halves, count, add):
    grads = refs[:halves]
    value_ref, gate_ref = refs[halves : halves + 2]
    out_ref = refs[-1]
    width = out_ref.shape[2]
    tok = out_ref.shape[1]
    block = tok // 4
    for i in range(count):
        rows = pl.ds(pl.multiple_of(index_ref[i] * width, 16), width)
        weight = []
        for h in range(halves):
            cols = pl.ds(h * LANE, LANE)
            weight += [value_ref[rows, cols], gate_ref[rows, cols]]
        weight = jnp.concatenate(weight, axis=1)
        for k in range(4):
            here = pl.ds(k * block, block)
            total = right_product(jnp.concatenate([g[here, :] for g in grads], axis=1), weight)
            if add:
                total = total + refs[halves + 2][index_ref[count + i], here, :].astype(f32)
            out_ref[i, here, :] = total.astype(bf16)


def input_blocks(grads, w_value, w_gate, blocks, n, got=None, got_block=None):
    halves = len(grads)
    t = grads[0].shape[0]
    d, c = w_value.shape
    width = d // n
    count = blocks.shape[0]
    index = blocks
    add = got is not None
    if add:
        index = jnp.concatenate([blocks, got_block])
    return pl.pallas_call(
        functools.partial(input_kernel, halves=halves, count=count, add=add),
        in_specs=[SMEM_SPEC] + [VMEM_SPEC] * (halves + 2 + add),
        out_specs=VMEM_SPEC,
        out_shape=jax.ShapeDtypeStruct((count, t, width), bf16),
        compiler_params=limit(16),
        cost_estimate=pl.CostEstimate(
            flops=4 * t * c * count * width,
            transcendentals=0,
            bytes_accessed=2 * (2 * t * c + 2 * count * width * c + count * t * width),
        ),
        name="input_blocks",
    )(index.astype(jnp.int32), *grads, w_value, w_gate, *([got] if add else []))


def input_gradient(grads, w_value, w_gate):
    n = lax.axis_size("tp")
    me = lax.axis_index("tp")
    half = n // 2
    high = jnp.arange(half)
    out = input_blocks(grads, w_value, w_gate, 2 * high + (me % 2 ^ 1), n)
    got = send(out, "tp", lambda i: i ^ 1)
    own = (me // 2).reshape(1)
    parts = []
    for k in range(1, half):
        other = (me // 2 ^ k).reshape(1)
        part = input_blocks(grads, w_value, w_gate, 2 * other + me % 2, n, got, other)
        parts.append(send(part, "tp", lambda i, k=k: i ^ (2 * k)))
    total = input_blocks(grads, w_value, w_gate, 2 * own + me % 2, n, got, own)[0].astype(f32)
    for part in parts:
        total = total + part[0].astype(f32)
    return total.astype(bf16)


def last_kernel(*refs, halves, pieces, scale):
    value_ref, gate_ref = refs[-2:]
    for h in range(halves):
        total = refs[h * pieces][...]
        for p in range(1, pieces):
            total = total + refs[h * pieces + p][...].astype(f32)
        total = total * scale
        cols = pl.ds(h * LANE, LANE)
        value_ref[:, cols] = total[:LANE].T
        gate_ref[:, cols] = total[LANE:].T


def last_sums(sums, scale):
    halves = len(sums)
    width = sums[0][0].shape[1]
    ch = halves * LANE
    if width % LANE:
        totals = [sum(p.astype(f32) for p in pieces) * scale for pieces in sums]
        return tuple(
            jnp.concatenate([t[m * LANE : (m + 1) * LANE] for t in totals], axis=0).T for m in range(2)
        )
    return pl.pallas_call(
        functools.partial(last_kernel, halves=halves, pieces=len(sums[0]), scale=scale),
        out_shape=[jax.ShapeDtypeStruct((width, ch), f32)] * 2,
        compiler_params=limit(10),
        name="last_sums",
    )(*(p for pieces in sums for p in pieces))


def work(block_input, out_grad, w_value, w_gate, conv_taps, norm_gain, norm_shift, w_proj):
    tok, _ = block_input.shape
    taps = conv_taps.shape[0]
    ch = w_value.shape[1]
    n_tp = lax.axis_size("tp")
    n_sp = lax.axis_size("sp")
    channels = ch * n_tp
    loss_scale = 1.0 / math.sqrt(tok * n_sp)
    value_proj, gate_proj, gated_input, own_mixed = project(
        block_input, w_value, w_gate, out_grad, w_proj, 4
    )
    after = send(jnp.concatenate([gated_input[:HALO].astype(f32), own_mixed[:HALO]], axis=0), "sp", lambda i: i - 1)
    before = send(gated_input[tok - HALO :], "sp", lambda i: i + 1)
    inner = convolve(gated_input, conv_taps)
    filtered = convolve_ends(inner, before, gated_input, after, conv_taps)
    stats = all_sum(row_sums(filtered, filtered * filtered), "tp")
    row_mean = stats[0] / channels
    row_scale = lax.rsqrt(stats[1] / channels - row_mean * row_mean + EPS)
    normed, grad_normed, turned, edge_sums = activate(
        filtered, as_columns([row_mean, row_scale]), own_mixed, after, norm_gain[None], norm_shift[None]
    )
    back = all_sum(row_sums(grad_normed, grad_normed * normed), "tp") / channels
    stats = as_columns([row_scale, back[0], back[1]])
    proj_parts, _ = reduce_blocks(turned, out_grad, last_first=True)
    halves = ch // LANE
    grads = []
    sums = []
    small = []
    for h in range(halves):
        grad, turn, tap_sums = back_convolve(
            normed, grad_normed, stats, before, gated_input, after, value_proj, gate_proj, conv_taps, h
        )
        grads.append(grad)
        small.append(tap_sums)
        rider = None
        if h == halves - 1:
            rider = jnp.concatenate([jnp.concatenate(small, axis=1), edge_sums], axis=0)
        parts, small_sum = reduce_blocks(turn, block_input, rider)
        sums.append(parts)
    kept = small[0].shape[0]
    input_grad = input_gradient(grads, w_value, w_gate)
    proj_wgrad = sum(p.astype(f32) for p in proj_parts) * loss_scale
    value_wgrad, gate_wgrad = last_sums(sums, loss_scale)
    return (
        input_grad,
        value_wgrad,
        gate_wgrad,
        proj_wgrad,
        small_sum[:taps] * loss_scale,
        small_sum[kept] * loss_scale,
        small_sum[kept + 1] * loss_scale,
    )


def solution(mesh):
    return mapped(mesh)


def mapped(mesh):
    return jax.shard_map(
        work,
        mesh=mesh,
        in_specs=(
            P("sp", None),
            P("sp", None),
            P(None, "tp"),
            P(None, "tp"),
            P(None, "tp"),
            P("tp"),
            P("tp"),
            P("tp", None),
        ),
        out_specs=(
            P("sp", "tp"),
            P("sp", "tp"),
            P("sp", "tp"),
            P("tp", "sp"),
            P(None, "tp"),
            P("tp"),
            P("tp"),
        ),
        check_vma=False,
    )
```

```python
import functools
import math

import jax
import jax.numpy as jnp
from jax import lax
from jax.experimental import pallas as pl
from jax.experimental.pallas import tpu as pltpu
from jax.sharding import PartitionSpec as P


EPS = 0.05
HALO = 32
LANE = 128
bf16 = jnp.bfloat16
f32 = jnp.float32


VMEM_SPEC = pl.BlockSpec(memory_space=pltpu.VMEM)
SMEM_SPEC = pl.BlockSpec(memory_space=pltpu.SMEM)
HBM_SPEC = pl.BlockSpec(memory_space=pltpu.HBM)


def limit(mib):
    return pltpu.CompilerParams(vmem_limit_bytes=mib * 1024 * 1024)


def send(block, axis, target):
    devices = range(lax.axis_size(axis))
    route = [(i, target(i)) for i in devices if 0 <= target(i) < len(devices)]
    return lax.ppermute(block, axis, route)


def all_sum(block, axis):
    step = 1
    while step < lax.axis_size(axis):
        block = block + send(block, axis, lambda i, b=step: i ^ b)
        step *= 2
    return block


def in_hbm(block):
    return pltpu.with_memory_space_constraint(block, pltpu.HBM)


def radices(size):
    out = []
    for r in (2, 4):
        if size % r == 0 and size > 1:
            out.append(r)
            size //= r
    if size > 1:
        out.append(size)
    return out


def right_product(left, right):
    return lax.dot_general(left, right, (((1,), (1,)), ((), ())), preferred_element_type=f32)


def blocks_kernel(ids_ref, left_ref, right_ref, *refs, gives):
    rider = refs[: -gives - 3]
    outs = refs[-gives - 3 : -3]
    own_hbm, own, sems = refs[-3:]
    rows = left_ref.shape[0]
    count, _, width = own.shape
    left = left_ref[...]

    def block(i):
        start = pl.multiple_of(ids_ref[i] * width, LANE)
        return jnp.dot(left, right_ref[:, pl.ds(start, width)], preferred_element_type=f32)

    leaving = [pltpu.make_async_copy(own.at[j], own_hbm.at[j], sems.at[j]) for j in range(count)]
    for j in range(count):
        own[j] = block(len(outs) * count + j)
        leaving[j].start()
    for i, out in enumerate(outs):
        for j in range(count):
            out[pl.ds(j * rows, rows), :] = block(i * count + j).astype(bf16)
        for m, extra in enumerate(rider):
            size = extra.shape[0]
            out[pl.ds(count * rows + m * size, size), :] = extra[...]
    for copy in leaving:
        copy.wait()


def grad_blocks(left, right, ids, n, rider):
    rows, tok = left.shape
    width = right.shape[1] // n
    count = ids[0].shape[0]
    gives = len(ids) - 1
    extra = sum(a.shape[0] for a in rider)
    if width % LANE:
        full = jnp.dot(left, right, preferred_element_type=f32).reshape(rows, n, width)
        full = full.transpose(1, 0, 2)
        outs = [jnp.take(full, some, axis=0) for some in ids]
        below = [a.reshape(-1, width) for a in rider]
        return [
            jnp.concatenate([o.astype(bf16).reshape(-1, width)] + below, axis=0) for o in outs[:-1]
        ] + outs[-1:]
    return pl.pallas_call(
        functools.partial(blocks_kernel, gives=gives),
        in_specs=[SMEM_SPEC] + [VMEM_SPEC] * (2 + len(rider)),
        out_specs=[VMEM_SPEC] * gives + [HBM_SPEC],
        out_shape=[jax.ShapeDtypeStruct((count * rows + extra, width), bf16)] * gives
        + [pltpu.HBM((count, rows, width), f32)],
        scratch_shapes=[pltpu.VMEM((count, rows, width), f32), pltpu.SemaphoreType.DMA((count,))],
        compiler_params=limit(10),
        cost_estimate=pl.CostEstimate(
            flops=2 * rows * tok * count * width * len(ids),
            transcendentals=0,
            bytes_accessed=2 * tok * (rows + count * width * len(ids)) + 4 * rows * count * width * len(ids),
        ),
        name="grad_blocks",
    )(jnp.concatenate(ids).astype(jnp.int32), left, right, *rider)


def shift(k, radix, stride):
    def target(i):
        own = (i // stride) % radix
        return i + ((own + k) % radix - own) * stride

    return target


def reduce_blocks(left, right, small=None, last_first=False):
    n = lax.axis_size("sp")
    me = lax.axis_index("sp")
    stages = []
    stride = 1
    for r in radices(n):
        stages.append((r, stride, (me // stride) % r))
        stride *= r
    if last_first:
        stages.reverse()
    base = jnp.zeros((1,), jnp.int32)
    for r, stride, _ in stages[1:]:
        base = (base[:, None] + stride * jnp.arange(r)[None]).reshape(-1)
    rest = tuple(r for r, _, _ in stages[1:])
    r, stride, digit = stages[0]
    rows = left.shape[0]
    width = right.shape[1] // n

    def ids(k):
        return base + (digit + k) % r * stride

    def split(message, above):
        return message[above:].astype(f32).reshape(small.shape)

    def total(own, got, digit, r):
        if r == 2:
            return own + got[0]
        pile = jnp.stack([own] + got)
        order = [
            lax.dynamic_index_in_dim(pile, (digit - j) % r, 0, keepdims=False) for j in range(r)
        ]
        return sum(order[1:], order[0])

    rider = [] if small is None else [small.astype(bf16)]
    *outs, own = grad_blocks(left, right, [ids(k) for k in range(1, r)] + [ids(0)], n, rider)
    got = [send(o, "sp", shift(k + 1, r, stride)) for k, o in enumerate(outs)]
    left_blocks = base.shape[0]
    if small is not None:
        riders = [split(g, left_blocks * rows) for g in got]
        small = total(rider[0].astype(f32), riders, digit, r)
    parts = [own.reshape(-1, width)] + got
    for r, stride, digit in stages[1:]:
        left_blocks //= r
        size = left_blocks * rows

        def pick(k):
            start = (digit + k) % r * size
            return sum(lax.dynamic_slice_in_dim(p, start, size, 0).astype(f32) for p in parts)

        sent = [pick(k).astype(bf16) for k in range(1, r)]
        if small is not None:
            rider = small.astype(bf16)
            below = rider.reshape(-1, width)
            sent = [jnp.concatenate([x, below], axis=0) for x in sent]
        got = [send(x, "sp", shift(k + 1, r, stride)) for k, x in enumerate(sent)]
        if small is not None:
            small = total(rider.astype(f32), [split(g, size) for g in got], digit, r)
        parts = [pick(0)] + got
    return [p[:rows] for p in parts], small


def project_kernel(
    x_hbm, wv_hbm, wg_hbm, g_hbm, wp_hbm, v_hbm, s_hbm, u_out, m_hbm, x_buf, g_buf, wv_buf, wg_buf, wp_buf, v_out, s_out, m_out, sems
):
    count, block, _ = x_buf.shape

    def copies(at, hbm, buf):
        return [
            pltpu.make_async_copy(hbm.at[pl.ds(k * block, block), :], buf.at[k], sems.at[at, k])
            for k in range(count)
        ]

    weights = [
        pltpu.make_async_copy(hbm, buf, sems.at[2, k])
        for k, (hbm, buf) in enumerate(((wv_hbm, wv_buf), (wg_hbm, wg_buf), (wp_hbm, wp_buf)))
    ]
    inputs = copies(0, x_hbm, x_buf)
    grads = copies(1, g_hbm, g_buf)
    for copy in weights[:2] + inputs + weights[2:] + grads:
        copy.start()
    weights[0].wait()
    weights[1].wait()
    for k in range(count):
        inputs[k].wait()
        rows = pl.ds(k * block, block)
        v = jnp.dot(x_buf[k], wv_buf[...], preferred_element_type=f32).astype(bf16)
        s = jnp.dot(x_buf[k], wg_buf[...], preferred_element_type=f32).astype(bf16)
        v_out[rows, :] = v
        s_out[rows, :] = s
        u_out[rows, :] = (v.astype(f32) * jax.nn.sigmoid(s.astype(f32))).astype(bf16)
    leaving = [
        pltpu.make_async_copy(v_out, v_hbm, sems.at[3, 0]),
        pltpu.make_async_copy(s_out, s_hbm, sems.at[3, 1]),
    ]
    for copy in leaving:
        copy.start()
    weights[2].wait()
    for k in range(count):
        grads[k].wait()
        rows = pl.ds(k * block, block)
        m_out[rows, :] = right_product(g_buf[k], wp_buf[...])
        leaving.append(pltpu.make_async_copy(m_out.at[rows, :], m_hbm.at[rows, :], sems.at[4, k]))
        leaving[-1].start()
    for copy in leaving:
        copy.wait()


def project(x, wv, wg, g, wp, count):
    t, d = x.shape
    c = wv.shape[1]
    hbm = pl.BlockSpec(memory_space=pl.ANY)
    return pl.pallas_call(
        project_kernel,
        in_specs=[hbm] * 5,
        out_specs=[HBM_SPEC] * 2 + [VMEM_SPEC, HBM_SPEC],
        out_shape=[pltpu.HBM((t, c), bf16)] * 2 + [jax.ShapeDtypeStruct((t, c), bf16), pltpu.HBM((t, c), f32)],
        scratch_shapes=[
            pltpu.VMEM((count, t // count, d), bf16),
            pltpu.VMEM((count, t // count, d), bf16),
            pltpu.VMEM((d, c), bf16),
            pltpu.VMEM((d, c), bf16),
            pltpu.VMEM((c, d), bf16),
            pltpu.VMEM((t, c), bf16),
            pltpu.VMEM((t, c), bf16),
            pltpu.VMEM((t, c), f32),
            pltpu.SemaphoreType.DMA((5, max(3, count))),
        ],
        compiler_params=limit(20),
        cost_estimate=pl.CostEstimate(
            flops=6 * t * d * c, transcendentals=t * c, bytes_accessed=2 * (2 * t * d + 3 * d * c + 5 * t * c)
        ),
        name="project",
    )(*(in_hbm(a) for a in (x, wv, wg, g, wp)))


def chunk_of(rows, most):
    return max(c for c in range(16, most + 1, 16) if rows % c == 0)


def fill_extended(ext_ref, before, glu, after, tok):
    ext_ref[pl.ds(0, HALO), :] = before.astype(f32)
    ext_ref[pl.ds(HALO, tok), :] = glu.astype(f32)
    ext_ref[pl.ds(HALO + tok, HALO), :] = after


def tap_rows(taps_ref, taps):
    return [jnp.broadcast_to(taps_ref[pl.ds(k, 1), :], (8, LANE)) for k in range(taps)]


def conv_rows(ext_ref, weights, base, chunk):
    x = ext_ref[pl.ds(base, chunk + HALO), :]
    acc = [None] * (chunk // 8)
    for r in range(8):
        moved = x if r == 0 else pltpu.roll(x, r, 0)
        for k in range(r, len(weights), 8):
            for j in range(chunk // 8):
                low = HALO + 8 * j - (k - r)
                part = weights[k] * moved[low : low + 8]
                acc[j] = part if acc[j] is None else acc[j] + part
    return acc


def conv_kernel(glu_ref, taps_ref, out_ref, wide_ref):
    tok = glu_ref.shape[0]
    rows = tok - HALO
    chunk = chunk_of(rows, 96)
    wide_ref[...] = glu_ref[...].astype(f32)
    weights = tap_rows(taps_ref, taps_ref.shape[0])

    def step(i, carry):
        base = pl.multiple_of(i * chunk, chunk)
        for j, part in enumerate(conv_rows(wide_ref, weights, base, chunk)):
            out_ref[pl.ds(base + HALO + 8 * j, 8), :] = part
        return carry

    lax.fori_loop(0, rows // chunk, step, 0)


def convolve(glu, conv_taps):
    tok, ch = glu.shape
    taps = conv_taps.shape[0]
    column = lambda i: (0, i)
    return pl.pallas_call(
        conv_kernel,
        grid=(ch // LANE,),
        in_specs=[pl.BlockSpec((tok, LANE), column), pl.BlockSpec((taps, LANE), column)],
        out_specs=pl.BlockSpec((tok + HALO, LANE), column),
        out_shape=jax.ShapeDtypeStruct((tok + HALO, ch), f32),
        scratch_shapes=[pltpu.VMEM((tok, LANE), f32)],
        compiler_params=limit(6),
        cost_estimate=pl.CostEstimate(
            flops=20 * taps * tok * ch, transcendentals=0, bytes_accessed=6 * tok * ch
        ),
        name="convolve",
    )(glu, conv_taps)


def ends_kernel(before_ref, head_ref, tail_ref, after_ref, taps_ref, main_ref, out_ref, ext_ref):
    ch = head_ref.shape[1]
    rows = main_ref.shape[0]
    for h in range(ch // LANE):
        cols = pl.ds(h * LANE, LANE)
        weights = [jnp.broadcast_to(taps_ref[pl.ds(k, 1), cols], (8, LANE)) for k in range(taps_ref.shape[0])]
        for m, (first, second) in enumerate(((before_ref, head_ref), (tail_ref, after_ref))):
            ext_ref[pl.ds(0, HALO), :] = first[:, cols].astype(f32)
            ext_ref[pl.ds(HALO, HALO), :] = second[pl.ds(0, HALO), cols].astype(f32)
            for j, part in enumerate(conv_rows(ext_ref, weights, 0, HALO)):
                out_ref[pl.ds(m * (rows - HALO) + 8 * j, 8), cols] = part


def convolve_ends(main, before, glu, after, conv_taps):
    return pl.pallas_call(
        ends_kernel,
        in_specs=[VMEM_SPEC] * 6,
        out_specs=VMEM_SPEC,
        out_shape=jax.ShapeDtypeStruct(main.shape, f32),
        input_output_aliases={5: 0},
        scratch_shapes=[pltpu.VMEM((2 * HALO, LANE), f32)],
        compiler_params=limit(4),
        cost_estimate=pl.CostEstimate(
            flops=80 * conv_taps.size * HALO, transcendentals=0, bytes_accessed=16 * HALO * main.shape[1]
        ),
        name="convolve_ends",
    )(before, glu[:HALO], glu[glu.shape[0] - HALO :], after, conv_taps, main)


def row_sums(first, second):
    pair = jnp.stack([jnp.sum(first, axis=1), jnp.sum(second, axis=1)])
    return jnp.pad(pair, ((0, 0), (0, -pair.shape[1] % LANE)))


def as_columns(rows):
    return jnp.pad(jnp.stack(rows), ((0, 8 - len(rows)), (0, 0)))


def act_kernel(
    filtered_ref, stats_ref, mixed_ref, edge_ref, gain_ref, shift_ref,
    normed_ref, grad_ref, turned_ref, sums_ref, col_ref, out_ref,
):
    ch = filtered_ref.shape[1]
    tok = mixed_ref.shape[0]
    col_ref[...] = stats_ref[...].T
    chunk = chunk_of(tok, 64)

    def some_rows(base, count, mixed, own):
        here = pl.ds(base, count)
        mean = jnp.broadcast_to(col_ref[here, pl.ds(0, 1)], (count, LANE))
        scale = jnp.broadcast_to(col_ref[here, pl.ds(1, 1)], (count, LANE))
        sums = []
        for h in range(ch // LANE):
            cols = pl.ds(h * LANE, LANE)
            normed = (filtered_ref[here, cols] - mean) * scale
            gain = gain_ref[:, cols]
            active = normed * gain + shift_ref[:, cols]
            s = jax.nn.sigmoid(active)
            act = mixed[:, h * LANE : (h + 1) * LANE] * s * (1.0 + active * (1.0 - s))
            normed_ref[here, cols] = normed
            grad_ref[here, cols] = act * gain
            if own:
                out_ref[here, cols] = (active * s).astype(bf16)
                sums.append(fold(act * normed))
                sums.append(fold(act))
        return sums

    def fold(x):
        total = x[0:8]
        for j in range(8, x.shape[0], 8):
            total = total + x[j : j + 8]
        return total

    def step(i, sums):
        base = pl.multiple_of(i * chunk, chunk)
        more = some_rows(base, chunk, mixed_ref[pl.ds(base, chunk), :], True)
        return tuple(a + b for a, b in zip(sums, more))

    zero = jnp.zeros((8, LANE), f32)
    sums = lax.fori_loop(0, tok // chunk, step, (zero,) * (2 * (ch // LANE)))
    some_rows(tok, HALO, edge_ref[...], False)
    sums_ref[...] = jnp.zeros_like(sums_ref)
    for h in range(ch // LANE):
        for m in range(2):
            sums_ref[pl.ds(m, 1), pl.ds(h * LANE, LANE)] = jnp.sum(sums[2 * h + m], axis=0, keepdims=True)
    for i in range(0, tok, LANE):
        turned_ref[:, pl.ds(i, LANE)] = out_ref[pl.ds(i, LANE), :].T


def activate(filtered, stats, mixed, after, gain, shift_row):
    rows, ch = filtered.shape
    tok = mixed.shape[0]
    wide = stats.shape[1]
    whole = lambda i: (0, 0)
    return pl.pallas_call(
        act_kernel,
        grid=(1,),
        in_specs=[
            pl.BlockSpec((rows, ch), whole),
            pl.BlockSpec((8, wide), whole),
            pl.BlockSpec((tok, ch), whole),
            pl.BlockSpec((HALO, ch), lambda i: (1, 0)),
            pl.BlockSpec((1, ch), whole),
            pl.BlockSpec((1, ch), whole),
        ],
        out_specs=[
            pl.BlockSpec((rows, ch), whole),
            pl.BlockSpec((rows, ch), whole),
            pl.BlockSpec((ch, tok), whole),
            pl.BlockSpec((16, ch), whole),
        ],
        out_shape=[
            jax.ShapeDtypeStruct((rows, ch), f32),
            jax.ShapeDtypeStruct((rows, ch), f32),
            jax.ShapeDtypeStruct((ch, tok), bf16),
            jax.ShapeDtypeStruct((16, ch), f32),
        ],
        scratch_shapes=[pltpu.VMEM((wide, 8), f32), pltpu.VMEM((tok, ch), bf16)],
        compiler_params=limit(12),
        cost_estimate=pl.CostEstimate(
            flops=200 * tok * ch, transcendentals=2 * tok * ch, bytes_accessed=18 * tok * ch
        ),
        name="activate",
    )(filtered, stats, mixed, after, gain, shift_row)


def back_conv_kernel(
    normed_ref, gn_ref, stats_ref, before_ref, glu_ref, after_ref, v_ref, s_ref, taps_ref,
    out_ref, turned_out, small_ref, ext_ref, grad_ref, col_ref, *leave,
):
    turned_ref = leave[0] if leave else turned_out
    tok = glu_ref.shape[0]
    rows = tok + HALO
    taps = taps_ref.shape[0]
    col_ref[...] = stats_ref[...].T
    fill_extended(ext_ref, before_ref[...], glu_ref[...], after_ref[...], tok)
    part_rows = chunk_of(rows, 96)

    def filtered_grad(i, carry):
        here = pl.ds(pl.multiple_of(i * part_rows, part_rows), part_rows)
        scale, first, second = (
            jnp.broadcast_to(col_ref[here, pl.ds(m, 1)], (part_rows, LANE)) for m in range(3)
        )
        grad_ref[here, :] = scale * (gn_ref[here, :] - first - normed_ref[here, :] * second)
        return carry

    lax.fori_loop(0, rows // part_rows, filtered_grad, 0)
    weights = tap_rows(taps_ref, taps)
    chunk = chunk_of(tok, 64)

    def spread(i, carry):
        base = pl.multiple_of(i * chunk, chunk)
        x = grad_ref[pl.ds(base, chunk + HALO), :]
        acc = [None] * (chunk // 8)
        for r in range(8):
            moved = x if r == 0 else pltpu.roll(x, chunk + HALO - r, 0)
            for k in range(r, taps, 8):
                for j in range(chunk // 8):
                    low = 8 * j + k - r
                    part = weights[k] * moved[low : low + 8]
                    acc[j] = part if acc[j] is None else acc[j] + part
        glu = jnp.concatenate(acc, axis=0)
        v = v_ref[pl.ds(base, chunk), :].astype(f32)
        s = jax.nn.sigmoid(s_ref[pl.ds(base, chunk), :].astype(f32))
        through = glu * s
        out_ref[pl.ds(base, chunk), pl.ds(0, LANE)] = through.astype(bf16)
        out_ref[pl.ds(base, chunk), pl.ds(LANE, LANE)] = (through * v * (1.0 - s)).astype(bf16)
        return carry

    lax.fori_loop(0, tok // chunk, spread, 0)
    for i in range(0, tok, LANE):
        turned_ref[:, pl.ds(i, LANE)] = out_ref[pl.ds(i, LANE), :].T
    if leave:
        leaving = pltpu.make_async_copy(turned_ref, turned_out, leave[1])
        leaving.start()

    width = chunk_of(tok, 32)

    def gather(i, sums):
        base = pl.multiple_of(i * width, width)
        g = grad_ref[pl.ds(base, width), :]
        x = ext_ref[pl.ds(base, width + HALO), :]
        sums = list(sums)
        for r in range(8):
            moved = x if r == 0 else pltpu.roll(x, r, 0)
            for k in range(r, taps, 8):
                for j in range(width // 8):
                    low = HALO + 8 * j - (k - r)
                    sums[k] = sums[k] + g[8 * j : 8 * j + 8] * moved[low : low + 8]
        return tuple(sums)

    zero = jnp.zeros((8, LANE), f32)
    sums = lax.fori_loop(0, tok // width, gather, (zero,) * taps)
    for k in range(taps):
        small_ref[pl.ds(k, 1), :] = jnp.sum(sums[k], axis=0, keepdims=True)
    for k in range(taps, small_ref.shape[0]):
        small_ref[pl.ds(k, 1), :] = jnp.zeros((1, LANE), f32)
    if leave:
        leaving.wait()


def back_convolve(normed, gn, stats, before, glu, after, v, s, conv_taps, h, leave):
    tok, _ = glu.shape
    taps = conv_taps.shape[0]
    wide = stats.shape[1]
    column = lambda i: (0, h)
    first = lambda i: (0, 0)
    kept = -(-taps // 8) * 8
    return pl.pallas_call(
        back_conv_kernel,
        grid=(1,),
        in_specs=[
            pl.BlockSpec((tok + HALO, LANE), column),
            pl.BlockSpec((tok + HALO, LANE), column),
            pl.BlockSpec((8, wide), first),
            pl.BlockSpec((HALO, LANE), column),
            pl.BlockSpec((tok, LANE), column),
            pl.BlockSpec((HALO, LANE), column),
            pl.BlockSpec((tok, LANE), column),
            pl.BlockSpec((tok, LANE), column),
            pl.BlockSpec((taps, LANE), column),
        ],
        out_specs=[
            pl.BlockSpec((tok, 2 * LANE), first),
            HBM_SPEC if leave else pl.BlockSpec((2 * LANE, tok), first),
            pl.BlockSpec((kept, LANE), first),
        ],
        out_shape=[
            jax.ShapeDtypeStruct((tok, 2 * LANE), bf16),
            (pltpu.HBM if leave else jax.ShapeDtypeStruct)((2 * LANE, tok), bf16),
            jax.ShapeDtypeStruct((kept, LANE), f32),
        ],
        scratch_shapes=[
            pltpu.VMEM((tok + 2 * HALO, LANE), f32),
            pltpu.VMEM((tok + HALO, LANE), f32),
            pltpu.VMEM((wide, 8), f32),
        ]
        + ([pltpu.VMEM((2 * LANE, tok), bf16), pltpu.SemaphoreType.DMA] if leave else []),
        compiler_params=limit(12),
        cost_estimate=pl.CostEstimate(
            flops=40 * taps * tok * LANE, transcendentals=0, bytes_accessed=16 * tok * LANE
        ),
        name="back_convolve",
    )(normed, gn, stats, before, glu, after, v, s, conv_taps)


def input_kernel(index_ref, *refs, halves, fetch):
    grads = refs[:halves]
    if fetch:
        value_hbm, gate_hbm, add_ref, out_ref, value_ref, gate_ref, sems = refs[halves:]
        copies = []
        for m, (hbm, ref) in enumerate(((value_hbm, value_ref), (gate_hbm, gate_ref))):
            start = pl.multiple_of(index_ref[0] * ref.shape[0], 16)
            copies.append(pltpu.make_async_copy(hbm.at[pl.ds(start, ref.shape[0]), :], ref, sems.at[m]))
        for copy in copies:
            copy.start()
        for copy in copies:
            copy.wait()
        rows = slice(None)
    else:
        value_ref, gate_ref, out_ref = refs[halves:]
        rows = pl.ds(pl.multiple_of(index_ref[0] * out_ref.shape[1], 16), out_ref.shape[1])
    weight = []
    for h in range(halves):
        cols = pl.ds(h * LANE, LANE)
        weight += [value_ref[rows, cols], gate_ref[rows, cols]]
    total = right_product(
        jnp.concatenate([g[...] for g in grads], axis=1), jnp.concatenate(weight, axis=1)
    )
    if fetch:
        total = total + add_ref[...]
    out_ref[...] = total.astype(out_ref.dtype)


def input_block(grads, value, gate, block, n, add=None):
    t = grads[0].shape[0]
    d, c = value.shape
    width = d // n
    fetch = add is not None
    weights = [pl.BlockSpec(memory_space=pl.ANY)] * 2 + [VMEM_SPEC] if fetch else [VMEM_SPEC] * 2
    scratch = [
        pltpu.VMEM((width, c), bf16),
        pltpu.VMEM((width, c), bf16),
        pltpu.SemaphoreType.DMA((2,)),
    ]
    return pl.pallas_call(
        functools.partial(input_kernel, halves=len(grads), fetch=fetch),
        in_specs=[SMEM_SPEC] + [VMEM_SPEC] * len(grads) + weights,
        out_specs=VMEM_SPEC,
        out_shape=jax.ShapeDtypeStruct((t, width), bf16 if fetch else f32),
        scratch_shapes=scratch if fetch else [],
        compiler_params=limit(14),
        cost_estimate=pl.CostEstimate(
            flops=4 * t * c * width, transcendentals=0, bytes_accessed=2 * (2 * t * c + 2 * width * c + 3 * t * width)
        ),
        name="input_block",
    )(block.reshape(1).astype(jnp.int32), *grads, value, gate, *([add] if fetch else []))


def input_gradient(grads, pair_grads, weights, pair_weights):
    n = lax.axis_size("tp")
    me = lax.axis_index("tp")

    def both(block):
        own = input_block(grads, *weights, block, n)
        return input_block(pair_grads, *pair_weights, block, n, own)

    parts = []
    for k in range(1, n // 2):
        parts.append(send(both(me ^ (2 * k)), "tp", lambda i, k=k: i ^ (2 * k)))
    total = both(me)
    for part in parts:
        total = total.astype(f32) + part.astype(f32)
    return total.astype(bf16)


def last_kernel(*refs, halves, pieces, scale):
    value_ref, gate_ref = refs[-2:]
    for h in range(halves):
        total = refs[h * pieces][...]
        for p in range(1, pieces):
            total = total + refs[h * pieces + p][...].astype(f32)
        total = total * scale
        cols = pl.ds(h * LANE, LANE)
        value_ref[:, cols] = total[:LANE].T
        gate_ref[:, cols] = total[LANE:].T


def last_sums(sums, scale):
    halves = len(sums)
    width = sums[0][0].shape[1]
    ch = halves * LANE
    if width % LANE:
        totals = [sum(p.astype(f32) for p in pieces) * scale for pieces in sums]
        return tuple(
            jnp.concatenate([t[m * LANE : (m + 1) * LANE] for t in totals], axis=0).T for m in range(2)
        )
    return pl.pallas_call(
        functools.partial(last_kernel, halves=halves, pieces=len(sums[0]), scale=scale),
        out_shape=[jax.ShapeDtypeStruct((width, ch), f32)] * 2,
        compiler_params=limit(10),
        name="last_sums",
    )(*(p for pieces in sums for p in pieces))


def work(block_input, out_grad, w_value, w_gate, conv_taps, norm_gain, norm_shift, w_proj):
    tok, _ = block_input.shape
    taps = conv_taps.shape[0]
    ch = w_value.shape[1]
    n_tp = lax.axis_size("tp")
    n_sp = lax.axis_size("sp")
    channels = ch * n_tp
    loss_scale = 1.0 / math.sqrt(tok * n_sp)
    value_proj, gate_proj, gated_input, own_mixed = project(
        block_input, w_value, w_gate, out_grad, w_proj, 4
    )
    after = send(jnp.concatenate([gated_input[:HALO].astype(f32), own_mixed[:HALO]], axis=0), "sp", lambda i: i - 1)
    before = send(gated_input[tok - HALO :], "sp", lambda i: i + 1)
    pair_value = send(w_value, "tp", lambda i: i ^ 1)
    pair_gate = send(w_gate, "tp", lambda i: i ^ 1)
    inner = convolve(gated_input, conv_taps)
    filtered = convolve_ends(inner, before, gated_input, after, conv_taps)
    stats = all_sum(row_sums(filtered, filtered * filtered), "tp")
    row_mean = stats[0] / channels
    row_scale = lax.rsqrt(stats[1] / channels - row_mean * row_mean + EPS)
    normed, grad_normed, turned, edge_sums = activate(
        filtered, as_columns([row_mean, row_scale]), own_mixed, after, norm_gain[None], norm_shift[None]
    )
    back = all_sum(row_sums(grad_normed, grad_normed * normed), "tp") / channels
    stats = as_columns([row_scale, back[0], back[1]])
    proj_parts, _ = reduce_blocks(turned, out_grad, last_first=True)
    halves = ch // LANE
    grads = []
    pair_grads = []
    sums = []
    small = []
    for h in range(halves):
        grad, turn, tap_sums = back_convolve(
            normed, grad_normed, stats, before, gated_input, after, value_proj, gate_proj, conv_taps, h, h > 0
        )
        grads.append(grad)
        pair_grads.append(send(grad, "tp", lambda i: i ^ 1))
        small.append(tap_sums)
        rider = None
        if h == halves - 1:
            rider = jnp.concatenate([jnp.concatenate(small, axis=1), edge_sums], axis=0)
        parts, small_sum = reduce_blocks(turn, block_input, rider)
        sums.append(parts)
    kept = small[0].shape[0]
    input_grad = input_gradient(grads, pair_grads, (w_value, w_gate), (pair_value, pair_gate))
    proj_wgrad = sum(p.astype(f32) for p in proj_parts) * loss_scale
    value_wgrad, gate_wgrad = last_sums(sums, loss_scale)
    return (
        input_grad,
        value_wgrad,
        gate_wgrad,
        proj_wgrad,
        small_sum[:taps] * loss_scale,
        small_sum[kept] * loss_scale,
        small_sum[kept + 1] * loss_scale,
    )


def solution(mesh):
    return mapped(mesh)


def mapped(mesh):
    return jax.shard_map(
        work,
        mesh=mesh,
        in_specs=(
            P("sp", None),
            P("sp", None),
            P(None, "tp"),
            P(None, "tp"),
            P(None, "tp"),
            P("tp"),
            P("tp"),
            P("tp", None),
        ),
        out_specs=(
            P("sp", "tp"),
            P("sp", "tp"),
            P("sp", "tp"),
            P("tp", "sp"),
            P(None, "tp"),
            P("tp"),
            P("tp"),
        ),
        check_vma=False,
    )
```

```python
import functools
import math

import jax
import jax.numpy as jnp
from jax import lax
from jax.experimental import pallas as pl
from jax.experimental.pallas import tpu as pltpu
from jax.sharding import PartitionSpec as P


EPS = 0.05
HALO = 32
LANE = 128
bf16 = jnp.bfloat16
f32 = jnp.float32


VMEM_SPEC = pl.BlockSpec(memory_space=pltpu.VMEM)
SMEM_SPEC = pl.BlockSpec(memory_space=pltpu.SMEM)
HBM_SPEC = pl.BlockSpec(memory_space=pltpu.HBM)


def limit(mib):
    return pltpu.CompilerParams(vmem_limit_bytes=mib * 1024 * 1024)


def send(block, axis, target):
    devices = range(lax.axis_size(axis))
    route = [(i, target(i)) for i in devices if 0 <= target(i) < len(devices)]
    return lax.ppermute(block, axis, route)


def all_sum(block, axis):
    step = 1
    while step < lax.axis_size(axis):
        block = block + send(block, axis, lambda i, b=step: i ^ b)
        step *= 2
    return block


def in_hbm(block):
    return pltpu.with_memory_space_constraint(block, pltpu.HBM)


def radices(size):
    out = []
    for r in (2, 4):
        if size % r == 0 and size > 1:
            out.append(r)
            size //= r
    if size > 1:
        out.append(size)
    return out


def right_product(left, right):
    return lax.dot_general(left, right, (((1,), (1,)), ((), ())), preferred_element_type=f32)


def blocks_kernel(ids_ref, left_ref, right_ref, *refs, gives):
    rider = refs[: -gives - 3]
    outs = refs[-gives - 3 : -3]
    own_hbm, own, sems = refs[-3:]
    rows = left_ref.shape[0]
    count, _, width = own.shape
    left = left_ref[...]

    def block(i):
        start = pl.multiple_of(ids_ref[i] * width, LANE)
        return jnp.dot(left, right_ref[:, pl.ds(start, width)], preferred_element_type=f32)

    leaving = [pltpu.make_async_copy(own.at[j], own_hbm.at[j], sems.at[j]) for j in range(count)]
    for j in range(count):
        own[j] = block(len(outs) * count + j)
        leaving[j].start()
    for i, out in enumerate(outs):
        for j in range(count):
            out[pl.ds(j * rows, rows), :] = block(i * count + j).astype(bf16)
        for m, extra in enumerate(rider):
            size = extra.shape[0]
            out[pl.ds(count * rows + m * size, size), :] = extra[...]
    for copy in leaving:
        copy.wait()


def grad_blocks(left, right, ids, n, rider):
    rows, tok = left.shape
    width = right.shape[1] // n
    count = ids[0].shape[0]
    gives = len(ids) - 1
    extra = sum(a.shape[0] for a in rider)
    if width % LANE:
        full = jnp.dot(left, right, preferred_element_type=f32).reshape(rows, n, width)
        full = full.transpose(1, 0, 2)
        outs = [jnp.take(full, some, axis=0) for some in ids]
        below = [a.reshape(-1, width) for a in rider]
        return [
            jnp.concatenate([o.astype(bf16).reshape(-1, width)] + below, axis=0) for o in outs[:-1]
        ] + outs[-1:]
    return pl.pallas_call(
        functools.partial(blocks_kernel, gives=gives),
        in_specs=[SMEM_SPEC] + [VMEM_SPEC] * (2 + len(rider)),
        out_specs=[VMEM_SPEC] * gives + [HBM_SPEC],
        out_shape=[jax.ShapeDtypeStruct((count * rows + extra, width), bf16)] * gives
        + [pltpu.HBM((count, rows, width), f32)],
        scratch_shapes=[pltpu.VMEM((count, rows, width), f32), pltpu.SemaphoreType.DMA((count,))],
        compiler_params=limit(10),
        cost_estimate=pl.CostEstimate(
            flops=2 * rows * tok * count * width * len(ids),
            transcendentals=0,
            bytes_accessed=2 * tok * (rows + count * width * len(ids)) + 4 * rows * count * width * len(ids),
        ),
        name="grad_blocks",
    )(jnp.concatenate(ids).astype(jnp.int32), left, right, *rider)


def shift(k, radix, stride):
    def target(i):
        own = (i // stride) % radix
        return i + ((own + k) % radix - own) * stride

    return target


def reduce_blocks(left, right, small=None, last_first=False):
    n = lax.axis_size("sp")
    me = lax.axis_index("sp")
    stages = []
    stride = 1
    for r in radices(n):
        stages.append((r, stride, (me // stride) % r))
        stride *= r
    if last_first:
        stages.reverse()
    base = jnp.zeros((1,), jnp.int32)
    for r, stride, _ in stages[1:]:
        base = (base[:, None] + stride * jnp.arange(r)[None]).reshape(-1)
    rest = tuple(r for r, _, _ in stages[1:])
    r, stride, digit = stages[0]
    rows = left.shape[0]
    width = right.shape[1] // n

    def ids(k):
        return base + (digit + k) % r * stride

    def split(message, above):
        return message[above:].astype(f32).reshape(small.shape)

    def total(own, got, digit, r):
        if r == 2:
            return own + got[0]
        pile = jnp.stack([own] + got)
        order = [
            lax.dynamic_index_in_dim(pile, (digit - j) % r, 0, keepdims=False) for j in range(r)
        ]
        return sum(order[1:], order[0])

    rider = [] if small is None else [small.astype(bf16)]
    *outs, own = grad_blocks(left, right, [ids(k) for k in range(1, r)] + [ids(0)], n, rider)
    got = [send(o, "sp", shift(k + 1, r, stride)) for k, o in enumerate(outs)]
    left_blocks = base.shape[0]
    if small is not None:
        riders = [split(g, left_blocks * rows) for g in got]
        small = total(rider[0].astype(f32), riders, digit, r)
    parts = [own.reshape(-1, width)] + got
    for r, stride, digit in stages[1:]:
        left_blocks //= r
        size = left_blocks * rows

        def pick(k):
            start = (digit + k) % r * size
            return sum(lax.dynamic_slice_in_dim(p, start, size, 0).astype(f32) for p in parts)

        sent = [pick(k).astype(bf16) for k in range(1, r)]
        if small is not None:
            rider = small.astype(bf16)
            below = rider.reshape(-1, width)
            sent = [jnp.concatenate([x, below], axis=0) for x in sent]
        got = [send(x, "sp", shift(k + 1, r, stride)) for k, x in enumerate(sent)]
        if small is not None:
            small = total(rider.astype(f32), [split(g, size) for g in got], digit, r)
        parts = [pick(0)] + got
    return [p[:rows] for p in parts], small


def project_kernel(
    x_hbm, wv_hbm, wg_hbm, g_hbm, wp_hbm, v_hbm, s_hbm, u_out, m_out, x_buf, g_buf, wv_buf, wg_buf, wp_buf, v_out, s_out, sems
):
    count, block, _ = x_buf.shape
    weights = [
        pltpu.make_async_copy(hbm, buf, sems.at[1, k])
        for k, (hbm, buf) in enumerate(((wv_hbm, wv_buf), (wg_hbm, wg_buf), (wp_hbm, wp_buf)))
    ]
    edge = pltpu.make_async_copy(g_hbm.at[pl.ds(0, HALO), :], g_buf, sems.at[2, 0])
    inputs = [
        pltpu.make_async_copy(x_hbm.at[pl.ds(k * block, block), :], x_buf.at[k], sems.at[0, k])
        for k in range(count)
    ]
    for copy in weights[:2] + inputs + weights[2:] + [edge]:
        copy.start()
    weights[0].wait()
    weights[1].wait()
    leaving = []
    for k in range(count):
        inputs[k].wait()
        rows = pl.ds(k * block, block)
        v = jnp.dot(x_buf[k], wv_buf[...], preferred_element_type=f32).astype(bf16)
        s = jnp.dot(x_buf[k], wg_buf[...], preferred_element_type=f32).astype(bf16)
        v_out[rows, :] = v
        s_out[rows, :] = s
        u_out[rows, :] = (v.astype(f32) * jax.nn.sigmoid(s.astype(f32))).astype(bf16)
        for at, (buf, hbm) in enumerate(((v_out, v_hbm), (s_out, s_hbm))):
            leaving.append(pltpu.make_async_copy(buf.at[rows, :], hbm.at[rows, :], sems.at[3 + at, k]))
            leaving[-1].start()
    weights[2].wait()
    edge.wait()
    m_out[...] = right_product(g_buf[...], wp_buf[...])
    for copy in leaving:
        copy.wait()


def project(x, wv, wg, g, wp, count):
    t, d = x.shape
    c = wv.shape[1]
    hbm = pl.BlockSpec(memory_space=pl.ANY)
    return pl.pallas_call(
        project_kernel,
        in_specs=[hbm] * 5,
        out_specs=[HBM_SPEC] * 2 + [VMEM_SPEC] * 2,
        out_shape=[pltpu.HBM((t, c), bf16)] * 2
        + [jax.ShapeDtypeStruct((t, c), bf16), jax.ShapeDtypeStruct((HALO, c), f32)],
        scratch_shapes=[
            pltpu.VMEM((count, t // count, d), bf16),
            pltpu.VMEM((HALO, d), bf16),
            pltpu.VMEM((d, c), bf16),
            pltpu.VMEM((d, c), bf16),
            pltpu.VMEM((c, d), bf16),
            pltpu.VMEM((t, c), bf16),
            pltpu.VMEM((t, c), bf16),
            pltpu.SemaphoreType.DMA((5, max(3, count))),
        ],
        compiler_params=limit(16),
        cost_estimate=pl.CostEstimate(
            flops=4 * t * d * c, transcendentals=t * c, bytes_accessed=2 * (t * d + 3 * d * c + 3 * t * c)
        ),
        name="project",
    )(*(in_hbm(a) for a in (x, wv, wg, g, wp)))


def back_kernel(g_ref, w_ref, out_ref):
    out_ref[...] = right_product(g_ref[...], w_ref[...])


def back_project(g, w):
    t, d = g.shape
    c = w.shape[0]
    return pl.pallas_call(
        back_kernel,
        in_specs=[VMEM_SPEC, VMEM_SPEC],
        out_specs=VMEM_SPEC,
        out_shape=jax.ShapeDtypeStruct((t, c), f32),
        compiler_params=limit(8),
        cost_estimate=pl.CostEstimate(
            flops=2 * t * d * c, transcendentals=0, bytes_accessed=2 * t * d + 2 * d * c + 4 * t * c
        ),
        name="back_project",
    )(g, w)


def chunk_of(rows, most):
    return max(c for c in range(16, most + 1, 16) if rows % c == 0)


def conv_rows(ext_ref, weights, base, chunk):
    x = ext_ref[pl.ds(base, chunk + HALO), :]
    acc = [None] * (chunk // 8)
    for r in range(8):
        moved = x if r == 0 else pltpu.roll(x, r, 0)
        for k in range(r, len(weights), 8):
            for j in range(chunk // 8):
                low = HALO + 8 * j - (k - r)
                part = weights[k] * moved[low : low + 8]
                acc[j] = part if acc[j] is None else acc[j] + part
    return acc


def tap_rows(taps_ref, cols):
    return [jnp.broadcast_to(taps_ref[pl.ds(k, 1), cols], (8, LANE)) for k in range(taps_ref.shape[0])]


def conv_kernel(glu_ref, taps_ref, out_ref, wide_ref):
    tok, ch = glu_ref.shape
    rows = tok - HALO
    chunk = chunk_of(rows, 96)
    for h in range(ch // LANE):
        cols = pl.ds(h * LANE, LANE)
        wide_ref[...] = glu_ref[:, cols].astype(f32)
        weights = tap_rows(taps_ref, cols)

        def step(i, carry):
            base = pl.multiple_of(i * chunk, chunk)
            for j, part in enumerate(conv_rows(wide_ref, weights, base, chunk)):
                out_ref[pl.ds(base + HALO + 8 * j, 8), cols] = part
            return carry

        lax.fori_loop(0, rows // chunk, step, 0)


def convolve(glu, conv_taps):
    tok, ch = glu.shape
    return pl.pallas_call(
        conv_kernel,
        in_specs=[VMEM_SPEC, VMEM_SPEC],
        out_specs=VMEM_SPEC,
        out_shape=jax.ShapeDtypeStruct((tok + HALO, ch), f32),
        scratch_shapes=[pltpu.VMEM((tok, LANE), f32)],
        compiler_params=limit(6),
        cost_estimate=pl.CostEstimate(
            flops=20 * conv_taps.shape[0] * tok * ch, transcendentals=0, bytes_accessed=6 * tok * ch
        ),
        name="convolve",
    )(glu, conv_taps)


def ends_kernel(before_ref, head_ref, tail_ref, after_ref, taps_ref, main_ref, out_ref, ext_ref):
    ch = head_ref.shape[1]
    rows = main_ref.shape[0]
    for h in range(ch // LANE):
        cols = pl.ds(h * LANE, LANE)
        weights = tap_rows(taps_ref, cols)
        for m, (first, second) in enumerate(((before_ref, head_ref), (tail_ref, after_ref))):
            ext_ref[pl.ds(0, HALO), :] = first[:, cols].astype(f32)
            ext_ref[pl.ds(HALO, HALO), :] = second[pl.ds(0, HALO), cols].astype(f32)
            for j, part in enumerate(conv_rows(ext_ref, weights, 0, HALO)):
                out_ref[pl.ds(m * (rows - HALO) + 8 * j, 8), cols] = part


def convolve_ends(main, before, glu, after, conv_taps):
    return pl.pallas_call(
        ends_kernel,
        in_specs=[VMEM_SPEC] * 6,
        out_specs=VMEM_SPEC,
        out_shape=jax.ShapeDtypeStruct(main.shape, f32),
        input_output_aliases={5: 0},
        scratch_shapes=[pltpu.VMEM((2 * HALO, LANE), f32)],
        compiler_params=limit(4),
        cost_estimate=pl.CostEstimate(
            flops=80 * conv_taps.size * HALO, transcendentals=0, bytes_accessed=16 * HALO * main.shape[1]
        ),
        name="convolve_ends",
    )(before, glu[:HALO], glu[glu.shape[0] - HALO :], after, conv_taps, main)


def row_sums(first, second):
    pair = jnp.stack([jnp.sum(first, axis=1), jnp.sum(second, axis=1)])
    return jnp.pad(pair, ((0, 0), (0, -pair.shape[1] % LANE)))


def as_columns(rows):
    return jnp.pad(jnp.stack(rows), ((0, 8 - len(rows)), (0, 0)))


def act_kernel(
    filtered_ref, stats_ref, mixed_ref, after_ref, gain_ref, shift_ref,
    normed_ref, grad_ref, turned_ref, sums_ref, col_ref, out_ref,
):
    ch = filtered_ref.shape[1]
    tok = mixed_ref.shape[0]
    col_ref[...] = stats_ref[...].T
    chunk = chunk_of(tok, 64)

    def some_rows(base, count, mixed, own):
        here = pl.ds(base, count)
        mean = jnp.broadcast_to(col_ref[here, pl.ds(0, 1)], (count, LANE))
        scale = jnp.broadcast_to(col_ref[here, pl.ds(1, 1)], (count, LANE))
        sums = []
        for h in range(ch // LANE):
            cols = pl.ds(h * LANE, LANE)
            normed = (filtered_ref[here, cols] - mean) * scale
            gain = gain_ref[:, cols]
            active = normed * gain + shift_ref[:, cols]
            s = jax.nn.sigmoid(active)
            act = mixed[:, h * LANE : (h + 1) * LANE] * s * (1.0 + active * (1.0 - s))
            normed_ref[here, cols] = normed
            grad_ref[here, cols] = act * gain
            if own:
                out_ref[here, cols] = (active * s).astype(bf16)
                sums.append(fold(act * normed))
                sums.append(fold(act))
        return sums

    def fold(x):
        total = x[0:8]
        for j in range(8, x.shape[0], 8):
            total = total + x[j : j + 8]
        return total

    def step(i, sums):
        base = pl.multiple_of(i * chunk, chunk)
        more = some_rows(base, chunk, mixed_ref[pl.ds(base, chunk), :], True)
        return tuple(a + b for a, b in zip(sums, more))

    zero = jnp.zeros((8, LANE), f32)
    sums = lax.fori_loop(0, tok // chunk, step, (zero,) * (2 * (ch // LANE)))
    some_rows(tok, HALO, after_ref[pl.ds(HALO, HALO), :], False)
    sums_ref[...] = jnp.zeros_like(sums_ref)
    for h in range(ch // LANE):
        for m in range(2):
            sums_ref[pl.ds(m, 1), pl.ds(h * LANE, LANE)] = jnp.sum(sums[2 * h + m], axis=0, keepdims=True)
    for i in range(0, tok, LANE):
        turned_ref[:, pl.ds(i, LANE)] = out_ref[pl.ds(i, LANE), :].T


def activate(filtered, stats, mixed, after, gain, shift_row):
    rows, ch = filtered.shape
    tok = mixed.shape[0]
    wide = stats.shape[1]
    return pl.pallas_call(
        act_kernel,
        in_specs=[VMEM_SPEC] * 6,
        out_specs=[VMEM_SPEC] * 4,
        out_shape=[
            jax.ShapeDtypeStruct((rows, ch), f32),
            jax.ShapeDtypeStruct((rows, ch), f32),
            jax.ShapeDtypeStruct((ch, tok), bf16),
            jax.ShapeDtypeStruct((16, ch), f32),
        ],
        scratch_shapes=[pltpu.VMEM((wide, 8), f32), pltpu.VMEM((tok, ch), bf16)],
        compiler_params=limit(12),
        cost_estimate=pl.CostEstimate(
            flops=200 * tok * ch, transcendentals=2 * tok * ch, bytes_accessed=18 * tok * ch
        ),
        name="activate",
    )(filtered, stats, mixed, after, gain, shift_row)


def back_conv_kernel(
    normed_ref, gn_ref, stats_ref, before_ref, glu_ref, after_ref, v_hbm, s_hbm, taps_ref,
    out_ref, turned_out, small_ref, ext_ref, grad_ref, col_ref, v_ref, s_ref, sems, *leave, h,
):
    turned_ref = leave[0] if leave else turned_out
    tok = glu_ref.shape[0]
    rows = tok + HALO
    taps = taps_ref.shape[0]
    cols = pl.ds(h * LANE, LANE)
    coming = [
        pltpu.make_async_copy(hbm.at[:, cols], ref, sems.at[m])
        for m, (hbm, ref) in enumerate(((v_hbm, v_ref), (s_hbm, s_ref)))
    ]
    for copy in coming:
        copy.start()
    col_ref[...] = stats_ref[...].T
    ext_ref[pl.ds(0, HALO), :] = before_ref[:, cols].astype(f32)
    ext_ref[pl.ds(HALO, tok), :] = glu_ref[:, cols].astype(f32)
    ext_ref[pl.ds(HALO + tok, HALO), :] = after_ref[pl.ds(0, HALO), cols]
    part_rows = chunk_of(rows, 96)

    def filtered_grad(i, carry):
        here = pl.ds(pl.multiple_of(i * part_rows, part_rows), part_rows)
        scale, first, second = (
            jnp.broadcast_to(col_ref[here, pl.ds(m, 1)], (part_rows, LANE)) for m in range(3)
        )
        grad_ref[here, :] = scale * (gn_ref[here, cols] - first - normed_ref[here, cols] * second)
        return carry

    lax.fori_loop(0, rows // part_rows, filtered_grad, 0)
    for copy in coming:
        copy.wait()
    weights = tap_rows(taps_ref, cols)
    chunk = chunk_of(tok, 128)

    def spread(i, carry):
        base = pl.multiple_of(i * chunk, chunk)
        x = grad_ref[pl.ds(base, chunk + HALO), :]
        acc = [None] * (chunk // 8)
        for r in range(8):
            moved = x if r == 0 else pltpu.roll(x, chunk + HALO - r, 0)
            for k in range(r, taps, 8):
                for j in range(chunk // 8):
                    low = 8 * j + k - r
                    part = weights[k] * moved[low : low + 8]
                    acc[j] = part if acc[j] is None else acc[j] + part
        glu = jnp.concatenate(acc, axis=0)
        v = v_ref[pl.ds(base, chunk), :].astype(f32)
        s = jax.nn.sigmoid(s_ref[pl.ds(base, chunk), :].astype(f32))
        through = glu * s
        out_ref[pl.ds(base, chunk), pl.ds(0, LANE)] = through.astype(bf16)
        out_ref[pl.ds(base, chunk), pl.ds(LANE, LANE)] = (through * v * (1.0 - s)).astype(bf16)
        return carry

    lax.fori_loop(0, tok // chunk, spread, 0)
    for i in range(0, tok, LANE):
        turned_ref[:, pl.ds(i, LANE)] = out_ref[pl.ds(i, LANE), :].T
    if leave:
        leaving = pltpu.make_async_copy(turned_ref, turned_out, leave[1])
        leaving.start()

    width = chunk_of(tok, 128)

    def gather(i, sums):
        base = pl.multiple_of(i * width, width)
        g = grad_ref[pl.ds(base, width), :]
        x = ext_ref[pl.ds(base, width + HALO), :]
        sums = list(sums)
        for r in range(8):
            moved = x if r == 0 else pltpu.roll(x, r, 0)
            for k in range(r, taps, 8):
                for j in range(width // 8):
                    low = HALO + 8 * j - (k - r)
                    sums[k] = sums[k] + g[8 * j : 8 * j + 8] * moved[low : low + 8]
        return tuple(sums)

    zero = jnp.zeros((8, LANE), f32)
    sums = lax.fori_loop(0, tok // width, gather, (zero,) * taps)
    for k in range(taps):
        small_ref[pl.ds(k, 1), :] = jnp.sum(sums[k], axis=0, keepdims=True)
    for k in range(taps, small_ref.shape[0]):
        small_ref[pl.ds(k, 1), :] = jnp.zeros((1, LANE), f32)
    if leave:
        leaving.wait()


def back_convolve(normed, gn, stats, before, glu, after, v, s, conv_taps, h, leave):
    tok, _ = glu.shape
    taps = conv_taps.shape[0]
    wide = stats.shape[1]
    kept = -(-taps // 8) * 8
    hbm = pl.BlockSpec(memory_space=pl.ANY)
    return pl.pallas_call(
        functools.partial(back_conv_kernel, h=h),
        in_specs=[VMEM_SPEC] * 6 + [hbm] * 2 + [VMEM_SPEC],
        out_specs=[VMEM_SPEC, HBM_SPEC if leave else VMEM_SPEC, VMEM_SPEC],
        out_shape=[
            jax.ShapeDtypeStruct((tok, 2 * LANE), bf16),
            (pltpu.HBM if leave else jax.ShapeDtypeStruct)((2 * LANE, tok), bf16),
            jax.ShapeDtypeStruct((kept, LANE), f32),
        ],
        scratch_shapes=[
            pltpu.VMEM((tok + 2 * HALO, LANE), f32),
            pltpu.VMEM((tok + HALO, LANE), f32),
            pltpu.VMEM((wide, 8), f32),
            pltpu.VMEM((tok, LANE), bf16),
            pltpu.VMEM((tok, LANE), bf16),
            pltpu.SemaphoreType.DMA((2,)),
        ]
        + ([pltpu.VMEM((2 * LANE, tok), bf16), pltpu.SemaphoreType.DMA] if leave else []),
        compiler_params=limit(12),
        cost_estimate=pl.CostEstimate(
            flops=40 * taps * tok * LANE, transcendentals=0, bytes_accessed=16 * tok * LANE
        ),
        name="back_convolve",
    )(normed, gn, stats, before, glu, after, v, s, conv_taps)


def input_kernel(index_ref, *refs, halves, fetch):
    grads = refs[:halves]
    if fetch:
        value_hbm, gate_hbm, add_ref, out_ref, value_ref, gate_ref, sems = refs[halves:]
        copies = []
        for m, (hbm, ref) in enumerate(((value_hbm, value_ref), (gate_hbm, gate_ref))):
            start = pl.multiple_of(index_ref[0] * ref.shape[0], 16)
            copies.append(pltpu.make_async_copy(hbm.at[pl.ds(start, ref.shape[0]), :], ref, sems.at[m]))
        for copy in copies:
            copy.start()
        for copy in copies:
            copy.wait()
        rows = slice(None)
    else:
        value_ref, gate_ref, out_ref = refs[halves:]
        rows = pl.ds(pl.multiple_of(index_ref[0] * out_ref.shape[1], 16), out_ref.shape[1])
    weight = []
    for h in range(halves):
        cols = pl.ds(h * LANE, LANE)
        weight += [value_ref[rows, cols], gate_ref[rows, cols]]
    total = right_product(
        jnp.concatenate([g[...] for g in grads], axis=1), jnp.concatenate(weight, axis=1)
    )
    if fetch:
        total = total + add_ref[...]
    out_ref[...] = total.astype(out_ref.dtype)


def input_block(grads, value, gate, block, n, add=None):
    t = grads[0].shape[0]
    d, c = value.shape
    width = d // n
    fetch = add is not None
    weights = [pl.BlockSpec(memory_space=pl.ANY)] * 2 + [VMEM_SPEC] if fetch else [VMEM_SPEC] * 2
    scratch = [
        pltpu.VMEM((width, c), bf16),
        pltpu.VMEM((width, c), bf16),
        pltpu.SemaphoreType.DMA((2,)),
    ]
    return pl.pallas_call(
        functools.partial(input_kernel, halves=len(grads), fetch=fetch),
        in_specs=[SMEM_SPEC] + [VMEM_SPEC] * len(grads) + weights,
        out_specs=VMEM_SPEC,
        out_shape=jax.ShapeDtypeStruct((t, width), bf16 if fetch else f32),
        scratch_shapes=scratch if fetch else [],
        compiler_params=limit(14),
        cost_estimate=pl.CostEstimate(
            flops=4 * t * c * width, transcendentals=0, bytes_accessed=2 * (2 * t * c + 2 * width * c + 3 * t * width)
        ),
        name="input_block",
    )(block.reshape(1).astype(jnp.int32), *grads, value, gate, *([add] if fetch else []))


def input_gradient(grads, pair_grads, weights, pair_weights):
    n = lax.axis_size("tp")
    me = lax.axis_index("tp")

    def both(block):
        own = input_block(grads, *weights, block, n)
        return input_block(pair_grads, *pair_weights, block, n, own)

    parts = []
    for k in range(1, n // 2):
        parts.append(send(both(me ^ (2 * k)), "tp", lambda i, k=k: i ^ (2 * k)))
    total = both(me)
    for part in parts:
        total = total.astype(f32) + part.astype(f32)
    return total.astype(bf16)


def last_kernel(*refs, halves, pieces, scale):
    value_ref, gate_ref = refs[-2:]
    for h in range(halves):
        total = refs[h * pieces][...]
        for p in range(1, pieces):
            total = total + refs[h * pieces + p][...].astype(f32)
        total = total * scale
        cols = pl.ds(h * LANE, LANE)
        value_ref[:, cols] = total[:LANE].T
        gate_ref[:, cols] = total[LANE:].T


def last_sums(sums, scale):
    halves = len(sums)
    width = sums[0][0].shape[1]
    ch = halves * LANE
    if width % LANE:
        totals = [sum(p.astype(f32) for p in pieces) * scale for pieces in sums]
        return tuple(
            jnp.concatenate([t[m * LANE : (m + 1) * LANE] for t in totals], axis=0).T for m in range(2)
        )
    return pl.pallas_call(
        functools.partial(last_kernel, halves=halves, pieces=len(sums[0]), scale=scale),
        out_shape=[jax.ShapeDtypeStruct((width, ch), f32)] * 2,
        compiler_params=limit(10),
        name="last_sums",
    )(*(p for pieces in sums for p in pieces))


def work(block_input, out_grad, w_value, w_gate, conv_taps, norm_gain, norm_shift, w_proj):
    tok, _ = block_input.shape
    taps = conv_taps.shape[0]
    ch = w_value.shape[1]
    n_tp = lax.axis_size("tp")
    n_sp = lax.axis_size("sp")
    channels = ch * n_tp
    loss_scale = 1.0 / math.sqrt(tok * n_sp)
    value_proj, gate_proj, gated_input, edge_mixed = project(
        block_input, w_value, w_gate, out_grad, w_proj, 4
    )
    after = send(jnp.concatenate([gated_input[:HALO].astype(f32), edge_mixed], axis=0), "sp", lambda i: i - 1)
    before = send(gated_input[tok - HALO :], "sp", lambda i: i + 1)
    pair_value = send(w_value, "tp", lambda i: i ^ 1)
    pair_gate = send(w_gate, "tp", lambda i: i ^ 1)
    inner = convolve(gated_input, conv_taps)
    filtered = convolve_ends(inner, before, gated_input, after, conv_taps)
    stats = all_sum(row_sums(filtered, filtered * filtered), "tp")
    own_mixed = back_project(out_grad, w_proj)
    row_mean = stats[0] / channels
    row_scale = lax.rsqrt(stats[1] / channels - row_mean * row_mean + EPS)
    normed, grad_normed, turned, edge_sums = activate(
        filtered, as_columns([row_mean, row_scale]), own_mixed, after, norm_gain[None], norm_shift[None]
    )
    back = all_sum(row_sums(grad_normed, grad_normed * normed), "tp") / channels
    stats = as_columns([row_scale, back[0], back[1]])
    proj_parts, _ = reduce_blocks(turned, out_grad, last_first=True)
    halves = ch // LANE
    grads = []
    pair_grads = []
    sums = []
    small = []
    for h in range(halves):
        grad, turn, tap_sums = back_convolve(
            normed, grad_normed, stats, before, gated_input, after, value_proj, gate_proj, conv_taps, h, False
        )
        grads.append(grad)
        pair_grads.append(send(grad, "tp", lambda i: i ^ 1))
        small.append(tap_sums)
        rider = None
        if h == halves - 1:
            rider = jnp.concatenate([jnp.concatenate(small, axis=1), edge_sums], axis=0)
        parts, small_sum = reduce_blocks(turn, block_input, rider)
        sums.append(parts)
    kept = small[0].shape[0]
    input_grad = input_gradient(grads, pair_grads, (w_value, w_gate), (pair_value, pair_gate))
    proj_wgrad = sum(p.astype(f32) for p in proj_parts) * loss_scale
    value_wgrad, gate_wgrad = last_sums(sums, loss_scale)
    return (
        input_grad,
        value_wgrad,
        gate_wgrad,
        proj_wgrad,
        small_sum[:taps] * loss_scale,
        small_sum[kept] * loss_scale,
        small_sum[kept + 1] * loss_scale,
    )


def solution(mesh):
    return mapped(mesh)


def mapped(mesh):
    return jax.shard_map(
        work,
        mesh=mesh,
        in_specs=(
            P("sp", None),
            P("sp", None),
            P(None, "tp"),
            P(None, "tp"),
            P(None, "tp"),
            P("tp"),
            P("tp"),
            P("tp", None),
        ),
        out_specs=(
            P("sp", "tp"),
            P("sp", "tp"),
            P("sp", "tp"),
            P("tp", "sp"),
            P(None, "tp"),
            P("tp"),
            P("tp"),
        ),
        check_vma=False,
    )
```

```python
import functools
import math

import jax
import jax.numpy as jnp
from jax import lax
from jax.experimental import pallas as pl
from jax.experimental.pallas import tpu as pltpu
from jax.sharding import PartitionSpec as P


EPS = 0.05
HALO = 32
LANE = 128
bf16 = jnp.bfloat16
f32 = jnp.float32


VMEM_SPEC = pl.BlockSpec(memory_space=pltpu.VMEM)
SMEM_SPEC = pl.BlockSpec(memory_space=pltpu.SMEM)
HBM_SPEC = pl.BlockSpec(memory_space=pltpu.HBM)


def limit(mib):
    return pltpu.CompilerParams(vmem_limit_bytes=mib * 1024 * 1024)


def send(block, axis, target):
    devices = range(lax.axis_size(axis))
    route = [(i, target(i)) for i in devices if 0 <= target(i) < len(devices)]
    return lax.ppermute(block, axis, route)


def all_sum(block, axis):
    step = 1
    while step < lax.axis_size(axis):
        block = block + send(block, axis, lambda i, b=step: i ^ b)
        step *= 2
    return block


def in_hbm(block):
    return pltpu.with_memory_space_constraint(block, pltpu.HBM)


def radices(size):
    out = []
    for r in (2, 4):
        if size % r == 0 and size > 1:
            out.append(r)
            size //= r
    if size > 1:
        out.append(size)
    return out


def right_product(left, right):
    return lax.dot_general(left, right, (((1,), (1,)), ((), ())), preferred_element_type=f32)


def blocks_kernel(ids_ref, left_ref, right_ref, *refs, gives):
    rider = refs[: -gives - 3]
    outs = refs[-gives - 3 : -3]
    own_hbm, own, sems = refs[-3:]
    rows = left_ref.shape[0]
    count, _, width = own.shape
    left = left_ref[...]

    def block(i):
        start = pl.multiple_of(ids_ref[i] * width, LANE)
        return jnp.dot(left, right_ref[:, pl.ds(start, width)], preferred_element_type=f32)

    leaving = [pltpu.make_async_copy(own.at[j], own_hbm.at[j], sems.at[j]) for j in range(count)]
    for j in range(count):
        own[j] = block(len(outs) * count + j).astype(bf16)
        leaving[j].start()
    for i, out in enumerate(outs):
        for j in range(count):
            out[pl.ds(j * rows, rows), :] = block(i * count + j).astype(bf16)
        for m, extra in enumerate(rider):
            size = extra.shape[0]
            out[pl.ds(count * rows + m * size, size), :] = extra[...]
    for copy in leaving:
        copy.wait()


def grad_blocks(left, right, ids, n, rider):
    rows, tok = left.shape
    width = right.shape[1] // n
    count = ids[0].shape[0]
    gives = len(ids) - 1
    extra = sum(a.shape[0] for a in rider)
    if width % LANE:
        full = jnp.dot(left, right, preferred_element_type=f32).reshape(rows, n, width)
        full = full.transpose(1, 0, 2)
        outs = [jnp.take(full, some, axis=0) for some in ids]
        below = [a.reshape(-1, width) for a in rider]
        return [
            jnp.concatenate([o.astype(bf16).reshape(-1, width)] + below, axis=0) for o in outs[:-1]
        ] + outs[-1:]
    return pl.pallas_call(
        functools.partial(blocks_kernel, gives=gives),
        in_specs=[SMEM_SPEC] + [VMEM_SPEC] * (2 + len(rider)),
        out_specs=[VMEM_SPEC] * gives + [HBM_SPEC],
        out_shape=[jax.ShapeDtypeStruct((count * rows + extra, width), bf16)] * gives
        + [pltpu.HBM((count, rows, width), bf16)],
        scratch_shapes=[pltpu.VMEM((count, rows, width), bf16), pltpu.SemaphoreType.DMA((count,))],
        compiler_params=limit(10),
        cost_estimate=pl.CostEstimate(
            flops=2 * rows * tok * count * width * len(ids),
            transcendentals=0,
            bytes_accessed=2 * tok * (rows + count * width * len(ids)) + 4 * rows * count * width * len(ids),
        ),
        name="grad_blocks",
    )(jnp.concatenate(ids).astype(jnp.int32), left, right, *rider)


def shift(k, radix, stride):
    def target(i):
        own = (i // stride) % radix
        return i + ((own + k) % radix - own) * stride

    return target


def reduce_blocks(left, right, small=None, last_first=False):
    n = lax.axis_size("sp")
    me = lax.axis_index("sp")
    stages = []
    stride = 1
    for r in radices(n):
        stages.append((r, stride, (me // stride) % r))
        stride *= r
    if last_first:
        stages.reverse()
    base = jnp.zeros((1,), jnp.int32)
    for r, stride, _ in stages[1:]:
        base = (base[:, None] + stride * jnp.arange(r)[None]).reshape(-1)
    rest = tuple(r for r, _, _ in stages[1:])
    r, stride, digit = stages[0]
    rows = left.shape[0]
    width = right.shape[1] // n

    def ids(k):
        return base + (digit + k) % r * stride

    def split(message, above):
        return message[above:].astype(f32).reshape(small.shape)

    def total(own, got, digit, r):
        if r == 2:
            return own + got[0]
        pile = jnp.stack([own] + got)
        order = [
            lax.dynamic_index_in_dim(pile, (digit - j) % r, 0, keepdims=False) for j in range(r)
        ]
        return sum(order[1:], order[0])

    rider = [] if small is None else [small.astype(bf16)]
    *outs, own = grad_blocks(left, right, [ids(k) for k in range(1, r)] + [ids(0)], n, rider)
    got = [send(o, "sp", shift(k + 1, r, stride)) for k, o in enumerate(outs)]
    left_blocks = base.shape[0]
    if small is not None:
        riders = [split(g, left_blocks * rows) for g in got]
        small = total(rider[0].astype(f32), riders, digit, r)
    parts = [own.reshape(-1, width)] + got
    for r, stride, digit in stages[1:]:
        left_blocks //= r
        size = left_blocks * rows

        def pick(k):
            start = (digit + k) % r * size
            return sum(lax.dynamic_slice_in_dim(p, start, size, 0).astype(f32) for p in parts)

        sent = [pick(k).astype(bf16) for k in range(1, r)]
        if small is not None:
            rider = small.astype(bf16)
            below = rider.reshape(-1, width)
            sent = [jnp.concatenate([x, below], axis=0) for x in sent]
        got = [send(x, "sp", shift(k + 1, r, stride)) for k, x in enumerate(sent)]
        if small is not None:
            small = total(rider.astype(f32), [split(g, size) for g in got], digit, r)
        parts = [pick(0)] + got
    return [p[:rows] for p in parts], small


def project_kernel(
    x_hbm, wv_hbm, wg_hbm, g_hbm, wp_hbm, v_hbm, s_hbm, u_out, m_out, x_buf, g_buf, wv_buf, wg_buf, wp_buf, v_out, s_out, sems
):
    count, block, _ = x_buf.shape
    weights = [
        pltpu.make_async_copy(hbm, buf, sems.at[1, k])
        for k, (hbm, buf) in enumerate(((wv_hbm, wv_buf), (wg_hbm, wg_buf), (wp_hbm, wp_buf)))
    ]
    edge = pltpu.make_async_copy(g_hbm.at[pl.ds(0, HALO), :], g_buf, sems.at[2, 0])
    inputs = [
        pltpu.make_async_copy(x_hbm.at[pl.ds(k * block, block), :], x_buf.at[k], sems.at[0, k])
        for k in range(count)
    ]
    for copy in weights[:2] + inputs + weights[2:] + [edge]:
        copy.start()
    weights[0].wait()
    weights[1].wait()
    leaving = []
    for k in range(count):
        inputs[k].wait()
        rows = pl.ds(k * block, block)
        v = jnp.dot(x_buf[k], wv_buf[...], preferred_element_type=f32).astype(bf16)
        s = jnp.dot(x_buf[k], wg_buf[...], preferred_element_type=f32).astype(bf16)
        v_out[rows, :] = v
        s_out[rows, :] = s
        u_out[rows, :] = (v.astype(f32) * jax.nn.sigmoid(s.astype(f32))).astype(bf16)
        for at, (buf, hbm) in enumerate(((v_out, v_hbm), (s_out, s_hbm))):
            leaving.append(pltpu.make_async_copy(buf.at[rows, :], hbm.at[rows, :], sems.at[3 + at, k]))
            leaving[-1].start()
    weights[2].wait()
    edge.wait()
    m_out[...] = right_product(g_buf[...], wp_buf[...])
    for copy in leaving:
        copy.wait()


def project(x, wv, wg, g, wp, count):
    t, d = x.shape
    c = wv.shape[1]
    hbm = pl.BlockSpec(memory_space=pl.ANY)
    return pl.pallas_call(
        project_kernel,
        in_specs=[hbm] * 5,
        out_specs=[HBM_SPEC] * 2 + [VMEM_SPEC] * 2,
        out_shape=[pltpu.HBM((t, c), bf16)] * 2
        + [jax.ShapeDtypeStruct((t, c), bf16), jax.ShapeDtypeStruct((HALO, c), f32)],
        scratch_shapes=[
            pltpu.VMEM((count, t // count, d), bf16),
            pltpu.VMEM((HALO, d), bf16),
            pltpu.VMEM((d, c), bf16),
            pltpu.VMEM((d, c), bf16),
            pltpu.VMEM((c, d), bf16),
            pltpu.VMEM((t, c), bf16),
            pltpu.VMEM((t, c), bf16),
            pltpu.SemaphoreType.DMA((5, max(3, count))),
        ],
        compiler_params=limit(16),
        cost_estimate=pl.CostEstimate(
            flops=4 * t * d * c, transcendentals=t * c, bytes_accessed=2 * (t * d + 3 * d * c + 3 * t * c)
        ),
        name="project",
    )(*(in_hbm(a) for a in (x, wv, wg, g, wp)))


def back_kernel(g_ref, w_ref, out_ref):
    out_ref[...] = right_product(g_ref[...], w_ref[...])


def back_project(g, w):
    t, d = g.shape
    c = w.shape[0]
    return pl.pallas_call(
        back_kernel,
        in_specs=[VMEM_SPEC, VMEM_SPEC],
        out_specs=VMEM_SPEC,
        out_shape=jax.ShapeDtypeStruct((t, c), f32),
        compiler_params=limit(8),
        cost_estimate=pl.CostEstimate(
            flops=2 * t * d * c, transcendentals=0, bytes_accessed=2 * t * d + 2 * d * c + 4 * t * c
        ),
        name="back_project",
    )(g, w)


def chunk_of(rows, most):
    return max(c for c in range(16, most + 1, 16) if rows % c == 0)


def conv_rows(ext_ref, weights, base, chunk):
    x = ext_ref[pl.ds(base, chunk + HALO), :]
    acc = [None] * (chunk // 8)
    for r in range(8):
        moved = x if r == 0 else pltpu.roll(x, r, 0)
        for k in range(r, len(weights), 8):
            for j in range(chunk // 8):
                low = HALO + 8 * j - (k - r)
                part = weights[k] * moved[low : low + 8]
                acc[j] = part if acc[j] is None else acc[j] + part
    return acc


def tap_rows(taps_ref, cols):
    return [jnp.broadcast_to(taps_ref[pl.ds(k, 1), cols], (8, LANE)) for k in range(taps_ref.shape[0])]


def conv_kernel(glu_ref, taps_ref, out_ref, wide_ref):
    tok, ch = glu_ref.shape
    rows = tok - HALO
    chunk = chunk_of(rows, 96)
    for h in range(ch // LANE):
        cols = pl.ds(h * LANE, LANE)
        wide_ref[...] = glu_ref[:, cols].astype(f32)
        weights = tap_rows(taps_ref, cols)

        def step(i, carry):
            base = pl.multiple_of(i * chunk, chunk)
            for j, part in enumerate(conv_rows(wide_ref, weights, base, chunk)):
                out_ref[pl.ds(base + HALO + 8 * j, 8), cols] = part
            return carry

        lax.fori_loop(0, rows // chunk, step, 0)


def convolve(glu, conv_taps):
    tok, ch = glu.shape
    return pl.pallas_call(
        conv_kernel,
        in_specs=[VMEM_SPEC, VMEM_SPEC],
        out_specs=VMEM_SPEC,
        out_shape=jax.ShapeDtypeStruct((tok + HALO, ch), f32),
        scratch_shapes=[pltpu.VMEM((tok, LANE), f32)],
        compiler_params=limit(6),
        cost_estimate=pl.CostEstimate(
            flops=20 * conv_taps.shape[0] * tok * ch, transcendentals=0, bytes_accessed=6 * tok * ch
        ),
        name="convolve",
    )(glu, conv_taps)


def ends_kernel(before_ref, head_ref, tail_ref, after_ref, taps_ref, main_ref, out_ref, ext_ref):
    ch = head_ref.shape[1]
    rows = main_ref.shape[0]
    for h in range(ch // LANE):
        cols = pl.ds(h * LANE, LANE)
        weights = tap_rows(taps_ref, cols)
        for m, (first, second) in enumerate(((before_ref, head_ref), (tail_ref, after_ref))):
            ext_ref[pl.ds(0, HALO), :] = first[:, cols].astype(f32)
            ext_ref[pl.ds(HALO, HALO), :] = second[pl.ds(0, HALO), cols].astype(f32)
            for j, part in enumerate(conv_rows(ext_ref, weights, 0, HALO)):
                out_ref[pl.ds(m * (rows - HALO) + 8 * j, 8), cols] = part


def convolve_ends(main, before, glu, after, conv_taps):
    return pl.pallas_call(
        ends_kernel,
        in_specs=[VMEM_SPEC] * 6,
        out_specs=VMEM_SPEC,
        out_shape=jax.ShapeDtypeStruct(main.shape, f32),
        input_output_aliases={5: 0},
        scratch_shapes=[pltpu.VMEM((2 * HALO, LANE), f32)],
        compiler_params=limit(4),
        cost_estimate=pl.CostEstimate(
            flops=80 * conv_taps.size * HALO, transcendentals=0, bytes_accessed=16 * HALO * main.shape[1]
        ),
        name="convolve_ends",
    )(before, glu[:HALO], glu[glu.shape[0] - HALO :], after, conv_taps, main)


def row_sums(first, second):
    pair = jnp.stack([jnp.sum(first, axis=1), jnp.sum(second, axis=1)])
    return jnp.pad(pair, ((0, 0), (0, -pair.shape[1] % LANE)))


def as_columns(rows):
    return jnp.pad(jnp.stack(rows), ((0, 8 - len(rows)), (0, 0)))


def act_kernel(
    filtered_ref, stats_ref, mixed_ref, after_ref, gain_ref, shift_ref,
    normed_ref, grad_ref, turned_ref, sums_ref, col_ref, out_ref,
):
    ch = filtered_ref.shape[1]
    tok = mixed_ref.shape[0]
    col_ref[...] = stats_ref[...].T
    chunk = chunk_of(tok, 128)

    def some_rows(base, count, mixed, own):
        here = pl.ds(base, count)
        mean = jnp.broadcast_to(col_ref[here, pl.ds(0, 1)], (count, LANE))
        scale = jnp.broadcast_to(col_ref[here, pl.ds(1, 1)], (count, LANE))
        sums = []
        for h in range(ch // LANE):
            cols = pl.ds(h * LANE, LANE)
            normed = (filtered_ref[here, cols] - mean) * scale
            gain = gain_ref[:, cols]
            active = normed * gain + shift_ref[:, cols]
            s = jax.nn.sigmoid(active)
            act = mixed[:, h * LANE : (h + 1) * LANE] * s * (1.0 + active * (1.0 - s))
            normed_ref[here, cols] = normed
            grad_ref[here, cols] = act * gain
            if own:
                out_ref[here, cols] = (active * s).astype(bf16)
                sums.append(fold(act * normed))
                sums.append(fold(act))
        return sums

    def fold(x):
        total = x[0:8]
        for j in range(8, x.shape[0], 8):
            total = total + x[j : j + 8]
        return total

    def step(i, sums):
        base = pl.multiple_of(i * chunk, chunk)
        more = some_rows(base, chunk, mixed_ref[pl.ds(base, chunk), :], True)
        return tuple(a + b for a, b in zip(sums, more))

    zero = jnp.zeros((8, LANE), f32)
    sums = lax.fori_loop(0, tok // chunk, step, (zero,) * (2 * (ch // LANE)))
    some_rows(tok, HALO, after_ref[pl.ds(HALO, HALO), :], False)
    sums_ref[...] = jnp.zeros_like(sums_ref)
    for h in range(ch // LANE):
        for m in range(2):
            sums_ref[pl.ds(m, 1), pl.ds(h * LANE, LANE)] = jnp.sum(sums[2 * h + m], axis=0, keepdims=True)
    for i in range(0, tok, LANE):
        turned_ref[:, pl.ds(i, LANE)] = out_ref[pl.ds(i, LANE), :].T


def activate(filtered, stats, mixed, after, gain, shift_row):
    rows, ch = filtered.shape
    tok = mixed.shape[0]
    wide = stats.shape[1]
    return pl.pallas_call(
        act_kernel,
        in_specs=[VMEM_SPEC] * 6,
        out_specs=[VMEM_SPEC] * 4,
        out_shape=[
            jax.ShapeDtypeStruct((rows, ch), f32),
            jax.ShapeDtypeStruct((rows, ch), f32),
            jax.ShapeDtypeStruct((ch, tok), bf16),
            jax.ShapeDtypeStruct((16, ch), f32),
        ],
        scratch_shapes=[pltpu.VMEM((wide, 8), f32), pltpu.VMEM((tok, ch), bf16)],
        compiler_params=limit(12),
        cost_estimate=pl.CostEstimate(
            flops=200 * tok * ch, transcendentals=2 * tok * ch, bytes_accessed=18 * tok * ch
        ),
        name="activate",
    )(filtered, stats, mixed, after, gain, shift_row)


def back_conv_kernel(
    normed_ref, gn_ref, stats_ref, before_ref, glu_ref, after_ref, v_hbm, s_hbm, taps_ref,
    out_ref, turned_out, small_ref, ext_ref, grad_ref, col_ref, v_ref, s_ref, sems, *leave, h,
):
    turned_ref = leave[0] if leave else turned_out
    tok = glu_ref.shape[0]
    rows = tok + HALO
    taps = taps_ref.shape[0]
    cols = pl.ds(h * LANE, LANE)
    coming = [
        pltpu.make_async_copy(hbm.at[:, cols], ref, sems.at[m])
        for m, (hbm, ref) in enumerate(((v_hbm, v_ref), (s_hbm, s_ref)))
    ]
    for copy in coming:
        copy.start()
    col_ref[...] = stats_ref[...].T
    ext_ref[pl.ds(0, HALO), :] = before_ref[:, cols].astype(f32)
    ext_ref[pl.ds(HALO, tok), :] = glu_ref[:, cols].astype(f32)
    ext_ref[pl.ds(HALO + tok, HALO), :] = after_ref[pl.ds(0, HALO), cols]
    part_rows = chunk_of(rows, 96)

    def filtered_grad(i, carry):
        here = pl.ds(pl.multiple_of(i * part_rows, part_rows), part_rows)
        scale, first, second = (
            jnp.broadcast_to(col_ref[here, pl.ds(m, 1)], (part_rows, LANE)) for m in range(3)
        )
        grad_ref[here, :] = scale * (gn_ref[here, cols] - first - normed_ref[here, cols] * second)
        return carry

    lax.fori_loop(0, rows // part_rows, filtered_grad, 0)
    width = chunk_of(tok, 128)

    def gather(i, sums):
        base = pl.multiple_of(i * width, width)
        g = grad_ref[pl.ds(base, width), :]
        x = ext_ref[pl.ds(base, width + HALO), :]
        sums = list(sums)
        for r in range(8):
            moved = x if r == 0 else pltpu.roll(x, r, 0)
            for k in range(r, taps, 8):
                for j in range(width // 8):
                    low = HALO + 8 * j - (k - r)
                    sums[k] = sums[k] + g[8 * j : 8 * j + 8] * moved[low : low + 8]
        return tuple(sums)

    zero = jnp.zeros((8, LANE), f32)
    sums = lax.fori_loop(0, tok // width, gather, (zero,) * taps)
    for k in range(taps):
        small_ref[pl.ds(k, 1), :] = jnp.sum(sums[k], axis=0, keepdims=True)
    for k in range(taps, small_ref.shape[0]):
        small_ref[pl.ds(k, 1), :] = jnp.zeros((1, LANE), f32)
    for copy in coming:
        copy.wait()
    weights = tap_rows(taps_ref, cols)
    chunk = chunk_of(tok, 128)

    def spread(i, carry):
        base = pl.multiple_of(i * chunk, chunk)
        x = grad_ref[pl.ds(base, chunk + HALO), :]
        acc = [None] * (chunk // 8)
        for r in range(8):
            moved = x if r == 0 else pltpu.roll(x, chunk + HALO - r, 0)
            for k in range(r, taps, 8):
                for j in range(chunk // 8):
                    low = 8 * j + k - r
                    part = weights[k] * moved[low : low + 8]
                    acc[j] = part if acc[j] is None else acc[j] + part
        glu = jnp.concatenate(acc, axis=0)
        v = v_ref[pl.ds(base, chunk), :].astype(f32)
        s = jax.nn.sigmoid(s_ref[pl.ds(base, chunk), :].astype(f32))
        through = glu * s
        out_ref[pl.ds(base, chunk), pl.ds(0, LANE)] = through.astype(bf16)
        out_ref[pl.ds(base, chunk), pl.ds(LANE, LANE)] = (through * v * (1.0 - s)).astype(bf16)
        return carry

    lax.fori_loop(0, tok // chunk, spread, 0)
    for i in range(0, tok, LANE):
        turned_ref[:, pl.ds(i, LANE)] = out_ref[pl.ds(i, LANE), :].T
    if leave:
        leaving = pltpu.make_async_copy(turned_ref, turned_out, leave[1])
        leaving.start()
    if leave:
        leaving.wait()


def back_convolve(normed, gn, stats, before, glu, after, v, s, conv_taps, h, leave):
    tok, _ = glu.shape
    taps = conv_taps.shape[0]
    wide = stats.shape[1]
    kept = -(-taps // 8) * 8
    hbm = pl.BlockSpec(memory_space=pl.ANY)
    return pl.pallas_call(
        functools.partial(back_conv_kernel, h=h),
        in_specs=[VMEM_SPEC] * 6 + [hbm] * 2 + [VMEM_SPEC],
        out_specs=[VMEM_SPEC, HBM_SPEC if leave else VMEM_SPEC, VMEM_SPEC],
        out_shape=[
            jax.ShapeDtypeStruct((tok, 2 * LANE), bf16),
            (pltpu.HBM if leave else jax.ShapeDtypeStruct)((2 * LANE, tok), bf16),
            jax.ShapeDtypeStruct((kept, LANE), f32),
        ],
        scratch_shapes=[
            pltpu.VMEM((tok + 2 * HALO, LANE), f32),
            pltpu.VMEM((tok + HALO, LANE), f32),
            pltpu.VMEM((wide, 8), f32),
            pltpu.VMEM((tok, LANE), bf16),
            pltpu.VMEM((tok, LANE), bf16),
            pltpu.SemaphoreType.DMA((2,)),
        ]
        + ([pltpu.VMEM((2 * LANE, tok), bf16), pltpu.SemaphoreType.DMA] if leave else []),
        compiler_params=limit(12),
        cost_estimate=pl.CostEstimate(
            flops=40 * taps * tok * LANE, transcendentals=0, bytes_accessed=16 * tok * LANE
        ),
        name="back_convolve",
    )(normed, gn, stats, before, glu, after, v, s, conv_taps)


def input_kernel(index_ref, *refs, halves):
    grads = refs[:halves]
    pair_grads = refs[halves : 2 * halves]
    value_ref, gate_ref, *pair_hbm, out_ref, pair_value, pair_gate, sems = refs[2 * halves :]
    _, width = out_ref.shape
    rows = pl.ds(pl.multiple_of(index_ref[0] * width, 16), width)
    copies = [
        pltpu.make_async_copy(hbm.at[rows, :], ref, sems.at[m])
        for m, (hbm, ref) in enumerate(zip(pair_hbm, (pair_value, pair_gate)))
    ]
    for copy in copies:
        copy.start()

    def product(grads, values, gates):
        weight = []
        for h in range(halves):
            cols = slice(h * LANE, (h + 1) * LANE)
            weight += [values[:, cols], gates[:, cols]]
        return right_product(
            jnp.concatenate([g[...] for g in grads], axis=1), jnp.concatenate(weight, axis=1)
        )

    total = product(grads, value_ref[rows, :], gate_ref[rows, :])
    for copy in copies:
        copy.wait()
    out_ref[...] = (total + product(pair_grads, pair_value[...], pair_gate[...])).astype(bf16)


def input_block(grads, pair_grads, weights, pair_weights, block, n):
    t = grads[0].shape[0]
    d, c = weights[0].shape
    width = d // n
    hbm = pl.BlockSpec(memory_space=pl.ANY)
    return pl.pallas_call(
        functools.partial(input_kernel, halves=len(grads)),
        in_specs=[SMEM_SPEC] + [VMEM_SPEC] * (2 * len(grads) + 2) + [hbm] * 2,
        out_specs=VMEM_SPEC,
        out_shape=jax.ShapeDtypeStruct((t, width), bf16),
        scratch_shapes=[
            pltpu.VMEM((width, c), bf16),
            pltpu.VMEM((width, c), bf16),
            pltpu.SemaphoreType.DMA((2,)),
        ],
        compiler_params=limit(16),
        cost_estimate=pl.CostEstimate(
            flops=8 * t * c * width, transcendentals=0, bytes_accessed=2 * (4 * t * c + 4 * width * c + t * width)
        ),
        name="input_block",
    )(block.reshape(1).astype(jnp.int32), *grads, *pair_grads, *weights, *pair_weights)


def input_gradient(grads, pair_grads, weights, pair_weights):
    n = lax.axis_size("tp")
    me = lax.axis_index("tp")

    def both(block):
        return input_block(grads, pair_grads, weights, pair_weights, block, n)

    parts = []
    for k in range(1, n // 2):
        parts.append(send(both(me ^ (2 * k)), "tp", lambda i, k=k: i ^ (2 * k)))
    total = both(me)
    for part in parts:
        total = total.astype(f32) + part.astype(f32)
    return total.astype(bf16)


def last_kernel(*refs, halves, pieces, scale):
    value_ref, gate_ref = refs[-2:]
    for h in range(halves):
        total = refs[h * pieces][...]
        for p in range(1, pieces):
            total = total + refs[h * pieces + p][...].astype(f32)
        total = total * scale
        cols = pl.ds(h * LANE, LANE)
        value_ref[:, cols] = total[:LANE].T
        gate_ref[:, cols] = total[LANE:].T


def last_sums(sums, scale):
    halves = len(sums)
    width = sums[0][0].shape[1]
    ch = halves * LANE
    if width % LANE:
        totals = [sum(p.astype(f32) for p in pieces) * scale for pieces in sums]
        return tuple(
            jnp.concatenate([t[m * LANE : (m + 1) * LANE] for t in totals], axis=0).T for m in range(2)
        )
    return pl.pallas_call(
        functools.partial(last_kernel, halves=halves, pieces=len(sums[0]), scale=scale),
        out_shape=[jax.ShapeDtypeStruct((width, ch), f32)] * 2,
        compiler_params=limit(10),
        name="last_sums",
    )(*(p for pieces in sums for p in pieces))


def work(block_input, out_grad, w_value, w_gate, conv_taps, norm_gain, norm_shift, w_proj):
    tok, _ = block_input.shape
    taps = conv_taps.shape[0]
    ch = w_value.shape[1]
    n_tp = lax.axis_size("tp")
    n_sp = lax.axis_size("sp")
    channels = ch * n_tp
    loss_scale = 1.0 / math.sqrt(tok * n_sp)
    value_proj, gate_proj, gated_input, edge_mixed = project(
        block_input, w_value, w_gate, out_grad, w_proj, 4
    )
    after = send(jnp.concatenate([gated_input[:HALO].astype(f32), edge_mixed], axis=0), "sp", lambda i: i - 1)
    before = send(gated_input[tok - HALO :], "sp", lambda i: i + 1)
    pair_value = send(w_value, "tp", lambda i: i ^ 1)
    pair_gate = send(w_gate, "tp", lambda i: i ^ 1)
    inner = convolve(gated_input, conv_taps)
    filtered = convolve_ends(inner, before, gated_input, after, conv_taps)
    stats = all_sum(row_sums(filtered, filtered * filtered), "tp")
    own_mixed = back_project(out_grad, w_proj)
    row_mean = stats[0] / channels
    row_scale = lax.rsqrt(stats[1] / channels - row_mean * row_mean + EPS)
    normed, grad_normed, turned, edge_sums = activate(
        filtered, as_columns([row_mean, row_scale]), own_mixed, after, norm_gain[None], norm_shift[None]
    )
    back = all_sum(row_sums(grad_normed, grad_normed * normed), "tp") / channels
    stats = as_columns([row_scale, back[0], back[1]])
    proj_parts, _ = reduce_blocks(turned, out_grad, last_first=True)
    halves = ch // LANE
    grads = []
    pair_grads = []
    sums = []
    small = []
    for h in range(halves):
        grad, turn, tap_sums = back_convolve(
            normed, grad_normed, stats, before, gated_input, after, value_proj, gate_proj, conv_taps, h, False
        )
        grads.append(grad)
        pair_grads.append(send(grad, "tp", lambda i: i ^ 1))
        small.append(tap_sums)
        rider = None
        if h == halves - 1:
            rider = jnp.concatenate([jnp.concatenate(small, axis=1), edge_sums], axis=0)
        parts, small_sum = reduce_blocks(turn, block_input, rider)
        sums.append(parts)
    kept = small[0].shape[0]
    input_grad = input_gradient(grads, pair_grads, (w_value, w_gate), (pair_value, pair_gate))
    proj_wgrad = sum(p.astype(f32) for p in proj_parts) * loss_scale
    value_wgrad, gate_wgrad = last_sums(sums, loss_scale)
    return (
        input_grad,
        value_wgrad,
        gate_wgrad,
        proj_wgrad,
        small_sum[:taps] * loss_scale,
        small_sum[kept] * loss_scale,
        small_sum[kept + 1] * loss_scale,
    )


def solution(mesh):
    return mapped(mesh)


def mapped(mesh):
    return jax.shard_map(
        work,
        mesh=mesh,
        in_specs=(
            P("sp", None),
            P("sp", None),
            P(None, "tp"),
            P(None, "tp"),
            P(None, "tp"),
            P("tp"),
            P("tp"),
            P("tp", None),
        ),
        out_specs=(
            P("sp", "tp"),
            P("sp", "tp"),
            P("sp", "tp"),
            P("tp", "sp"),
            P(None, "tp"),
            P("tp"),
            P("tp"),
        ),
        check_vma=False,
    )
```
